256 devices in a mesh: ep: 64 (over z, x, core), tp: 4 (over y).
Axes of the slice: x: 4, y: 4, z: 8, core: 2. Of those that a mesh axis runs over, the one named last changes fastest.
Arguments:
- first_micro_values: bfloat16 [65536, 2048], P('ep', 'tp'), may hold values from -6 to 6
- group_state_maps: bfloat16 [2, 65536, 1024], P(None, 'ep', 'tp'), may hold values from -6 to 6
- gate_preactivation: bfloat16 [65536, 2048], P('ep', 'tp'), may hold values from -6 to 6
- step_preactivation: float32 [65536, 32], P('ep', 'tp'), may hold values from -5.7 to 5.7
- head_step_bias: float32 [32], P('tp'), may hold values from -12 to -3
- head_log_decay: float32 [32], P('tp'), may hold values from -12 to 1
- decay_increment: float32 [65536, 32], P('ep', 'tp'), may hold values from -1.4 to 0
- head_direct_gain: float32 [32], P('tp'), may hold values from 0.1 to 1.9
- convolution_value_taps: bfloat16 [4, 2048], P(None, 'tp'), may hold values from -3 to 3
- convolution_map_taps: bfloat16 [2, 4, 1024], P(None, None, 'tp'), may hold values from -3 to 3
- grouped_norm_gain: float32 [2048], P('tp'), may hold values from 0.1 to 1.9
- second_micro_tokens: bfloat16 [65536, 2048], P(('ep', 'tp')), may hold values from -6 to 6
- expert_norm_gain: float32 [2048], replicated, may hold values from 0.1 to 1.9
- routes: int32 [65536, 2], P(('ep', 'tp')), may hold values from 0 to 63, all different within a row; in each aligned block of 256 rows (0 to 255, 256 to 511, ...) at most 12 rows name the same one
- visit_weight: float32 [65536, 2], P(('ep', 'tp')), may hold values from 0.1 to 1
- gate_weight_table: bfloat16 [64, 2048, 1024], P('ep', None, 'tp'), may hold values from -0.125 to 0.125
- up_weight_table: bfloat16 [64, 2048, 1024], P('ep', None, 'tp'), may hold values from -0.125 to 0.125
- down_weight_table: bfloat16 [64, 2048, 1024], P('ep', None, 'tp'), may hold values from -0.1875 to 0.1875
Outputs:
- mixer_gated_output: bfloat16 [65536, 2048], P('ep', 'tp')
- routed_out: bfloat16 [65536, 2048], P(('ep', 'tp'))
The draws below stay inside these ranges and needn't reach their ends.
Inputs may be any that keep to these rules, and one draw needn't show every extreme that they name: `routes`: A row names 2 different experts. In each aligned block of 256 rows (the rows of one device), no expert is named by more than 12 rows, a bound that some block reaches.
All inputs are finite; a program needn't handle non-finite values.
Results may differ from the reference program's by a relative error of at most 0.0071.
Values may be sent and summed in bfloat16 or wider, within the bound.
A program may use at most 128 MiB of HBM per device.

```python
import math
import jax
import jax.numpy as jnp
import numpy as np
from jax import lax

D = 2048
FF = 1024
HEADS = 32
HEADDIM = 64
GROUPS = 8
NSTATE = 128
CONV = 4
BLOCK = 128
TOPK = 2
TOK_DEV = 256
SEQ_DEV = 1024
SEQ = 65536
TOKENS = 65536
EXPERTS = 64
CAP = 12
INNER = 2048
N_EP = 64
N_TP = 4


def fast_heads(key):
    fast_share = 0.5
    return jax.random.uniform(jax.random.fold_in(key, 71), (HEADS,), jnp.float32) < fast_share


def draw_head_step_bias(key, part):
    fast_mask = fast_heads(key)
    jitter = jax.random.uniform(jax.random.fold_in(key, 72), (HEADS,), jnp.float32, -0.3, 0.3)
    slow_level = jnp.log(0.25 / jnp.sqrt(jnp.float32(SEQ)))
    return jnp.where(fast_mask, jnp.log(jnp.float32(0.02)), slow_level) + jitter


def draw_head_log_decay(key, part):
    fast_mask = fast_heads(key)
    jitter = jax.random.uniform(jax.random.fold_in(key, 73), (HEADS,), jnp.float32, -0.3, 0.3)
    slow_level = jnp.log(2.0 / jnp.sqrt(jnp.float32(SEQ)))
    return jnp.where(fast_mask, jnp.log(jnp.float32(1.5)), slow_level) + jitter


def draw_step_preactivation(key, part):
    noise_part = jnp.clip(jax.random.normal(jax.random.fold_in(key, 81), (SEQ, HEADS), jnp.float32), -5.0, 5.0)
    offsets = jax.random.uniform(jax.random.fold_in(key, 82), (SEQ // SEQ_DEV, HEADS), jnp.float32, -0.7, 0.7)
    return noise_part + jnp.repeat(offsets, SEQ_DEV, axis=0)


def draw_decay_increment(key, part):
    position_list = jax.random.randint(jax.random.fold_in(key, 91), (2, HEADS), 0, SEQ, dtype=jnp.int32)
    error_terms = jnp.log(jax.random.uniform(jax.random.fold_in(key, 92), (2, HEADS), jnp.float32, 0.5, 0.8))
    sequence_position_index = jnp.arange(SEQ, dtype=jnp.int32)[:, None]
    summed_total = jnp.zeros((SEQ, HEADS), jnp.float32)
    for spike_index in range(2):
        summed_total = summed_total + jnp.where(sequence_position_index == position_list[spike_index][None, :], error_terms[spike_index][None, :], 0.0)
    return summed_total


def shard_levels(own_key, dims, cuts, smallest, top_value):
    loudness, own = 1.0, jax.random.fold_in(own_key, 6)
    for axis_at, parts in cuts:
        steps = jnp.exp(jax.random.uniform(jax.random.fold_in(own, axis_at), (parts,), jnp.float32, smallest / len(cuts), top_value / len(cuts)))
        loudness = loudness * jnp.repeat(steps, dims[axis_at] // parts).reshape([-1 if axis == axis_at else 1 for axis in range(len(dims))])
    return loudness


def deal_out(key, own, number, rows, number_of, top, most, lean):
    order = jax.random.permutation(key, number_of)
    crowded, common = portions_of(number_of, rows * top, most, lean, True), portions_of(number_of, rows * top, most, lean, False)
    places = jnp.arange(number_of)

    def named(sizes, offset_by):
        used = int((sizes > 0).sum())
        fixed = max(1, used // 4)
        shifted = fixed + (places - fixed + offset_by * (used - fixed)) % max(1, number_of - fixed)
        return jnp.zeros((number_of,), jnp.int32).at[order[jnp.where(places < fixed, places, shifted)]].set(jnp.asarray(sizes, jnp.int32))

    sizes = jnp.where(number % 4 == 0, named(crowded, number // 4), named(common, number - number // 4 - 1))
    mixed = jax.random.permutation(jax.random.fold_in(own, 3), number_of)
    giver, sink = mixed[0:number_of // 2 * 2:2], mixed[1:number_of // 2 * 2:2]
    slack = jnp.minimum(sizes[giver] - 1, most - sizes[sink]) // 2
    slack = jnp.where((giver == order[0]) | (sink == order[0]) | (sizes[sink] == 0), 0, jnp.maximum(slack, 0))
    shifted = jax.random.randint(jax.random.fold_in(own, 4), (number_of // 2,), 0, 1 << 20) % (slack + 1)
    sizes = sizes.at[giver].add(-shifted).at[sink].add(shifted)
    labels = jnp.searchsorted(jnp.cumsum(sizes), jnp.arange(rows * top), side="right").astype(jnp.int32)
    table = labels.reshape(top, rows).T
    table = table[jax.random.permutation(jax.random.fold_in(own, 1), rows)]
    offset_by = jax.random.randint(jax.random.fold_in(own, 2), (rows, 1), 0, top)
    return jnp.take_along_axis(table, (jnp.arange(top)[None, :] + offset_by) % top, axis=1)


def portions_of(number_of, total, bound, skew, full):
    portions = [(1 << 20) // math.isqrt(rank ** skew) + 1 for rank in range(1, number_of + 1)]
    largest = bound if full else min(bound, max(-(-total // number_of), total * portions[0] // sum(portions)))
    least = 1 if total - largest >= number_of - 1 else 0
    counts, spare = [largest] + [least] * (number_of - 1), total - largest - least * (number_of - 1)
    while spare > 0:
        movable = [i for i in range(1, number_of) if counts[i] < largest] or [i for i in range(1, number_of) if counts[i] < bound]
        whole, budget = sum([portions[i] for i in movable]), spare
        for i in movable:
            extra = min(bound - counts[i], max(1, budget * portions[i] // whole), spare)
            counts[i] = counts[i] + extra
            spare = spare - extra
    return np.array(counts)


def bell_draw(own_key, dims, deviation, most, split=(), kind=jnp.bfloat16):
    values = jax.random.normal(own_key, dims, jnp.float32) * deviation
    if len(split) > 0:
        values = shard_levels(own_key, dims, split, -0.22, 0.18) * values
    return jnp.clip(values, min=-most, max=most).astype(kind)


def setup_inputs(seed: int = 0) -> dict:
    key_of = jax.random.split(jax.random.key(seed), 19)
    first_micro_values = bell_draw(key_of[0], (SEQ, INNER), 1.0, 6.0, ((0, 64), (1, 4)))
    group_state_maps = bell_draw(key_of[1], (2, SEQ, GROUPS * NSTATE), 1.0, 6.0, ((1, 64), (2, 4)))
    gate_preactivation = bell_draw(key_of[2], (SEQ, INNER), 1.0, 6.0, ((0, 64), (1, 4)))
    step_preactivation = draw_step_preactivation(jax.random.fold_in(key_of[18], 71), 0)
    head_step_bias = draw_head_step_bias(jax.random.fold_in(key_of[18], 71), 0)
    head_log_decay = draw_head_log_decay(jax.random.fold_in(key_of[18], 71), 0)
    decay_increment = draw_decay_increment(jax.random.fold_in(key_of[18], 71), 0)
    head_direct_gain = jnp.clip(1.0 + 0.18 * jax.random.normal(key_of[7], (HEADS,), jnp.float32), 0.1, 1.9)
    convolution_value_taps = bell_draw(key_of[8], (CONV, INNER), CONV ** -0.5, 3.0, ((1, 4),))
    convolution_map_taps = bell_draw(key_of[9], (2, CONV, GROUPS * NSTATE), CONV ** -0.5, 3.0, ((2, 4),))
    grouped_norm_gain = jnp.clip(1.0 + 0.18 * jax.random.normal(key_of[10], (INNER,), jnp.float32), 0.1, 1.9)
    second_micro_tokens = bell_draw(key_of[11], (TOKENS, D), 1.0, 6.0, ((0, 256),))
    expert_norm_gain = jnp.clip(1.0 + 0.18 * jax.random.normal(key_of[12], (D,), jnp.float32), 0.1, 1.9)
    routes_keys = jax.random.split(jax.random.fold_in(key_of[13], 1), TOKENS // TOK_DEV)
    routes_turns = jax.random.permutation(jax.random.fold_in(key_of[13], 3), TOKENS // TOK_DEV)
    routes = jax.vmap(lambda own, number: deal_out(jax.random.fold_in(key_of[13], 2), own, number, TOK_DEV, EXPERTS, TOPK, CAP, 0))(routes_keys, routes_turns).reshape((TOKENS, TOPK))
    visit_weight = jnp.clip(0.1 + 0.9 * jax.random.uniform(key_of[14], (TOKENS, TOPK), jnp.float32) ** shard_levels(key_of[14], (TOKENS, TOPK), ((0, 256),), -0.2, 0.2), 0.1, 1.0)
    gate_weight_table = bell_draw(key_of[15], (EXPERTS, D, FF), D ** -0.5, 0.125, ((0, 64), (2, 4)))
    up_weight_table = bell_draw(key_of[16], (EXPERTS, D, FF), D ** -0.5, 0.125, ((0, 64), (2, 4)))
    down_weight_table = bell_draw(key_of[17], (EXPERTS, D, FF), FF ** -0.5, 0.1875, ((0, 64), (2, 4)))
    return dict(first_micro_values=first_micro_values, group_state_maps=group_state_maps, gate_preactivation=gate_preactivation, step_preactivation=step_preactivation, head_step_bias=head_step_bias, head_log_decay=head_log_decay, decay_increment=decay_increment, head_direct_gain=head_direct_gain, convolution_value_taps=convolution_value_taps, convolution_map_taps=convolution_map_taps, grouped_norm_gain=grouped_norm_gain, second_micro_tokens=second_micro_tokens, expert_norm_gain=expert_norm_gain, routes=routes, visit_weight=visit_weight, gate_weight_table=gate_weight_table, up_weight_table=up_weight_table, down_weight_table=down_weight_table)


HIGHEST = lax.Precision.HIGHEST
EPSILON = 1e-05

def causal_conv(values, weights):
    length = values.shape[0]
    kernel = weights.shape[0]
    padded = jnp.pad(values.astype(jnp.float32), ((kernel - 1, 0), (0, 0)))
    summed_total = jnp.zeros(values.shape, jnp.float32)
    for offset in range(kernel):
        summed_total = summed_total + weights[offset].astype(jnp.float32) * padded[offset:offset + length]
    return jax.nn.silu(summed_total)

def mixer_baseline(first_micro_values, group_state_maps, gate_preactivation, step_preactivation, head_step_bias, head_log_decay, decay_increment, head_direct_gain, convolution_value_taps, convolution_map_taps, grouped_norm_gain):
    length, channels = first_micro_values.shape
    head_count = step_preactivation.shape[1]
    per_group = head_count // GROUPS
    blocks = length // BLOCK
    conv_out = causal_conv(first_micro_values, convolution_value_taps)
    in_maps = causal_conv(group_state_maps[0], convolution_map_taps[0])
    out_maps = causal_conv(group_state_maps[1], convolution_map_taps[1])
    step_length = jax.nn.softplus(step_preactivation + head_step_bias)
    decay_logarithm = -jnp.exp(head_log_decay) * step_length + decay_increment
    head_values = conv_out.reshape(blocks, BLOCK, GROUPS, per_group, HEADDIM)
    scaled_values = head_values * step_length.reshape(blocks, BLOCK, GROUPS, per_group)[..., None]
    in_blocks = in_maps.reshape(blocks, BLOCK, GROUPS, NSTATE)
    out_blocks = out_maps.reshape(blocks, BLOCK, GROUPS, NSTATE)
    running = jnp.cumsum(decay_logarithm.reshape(blocks, BLOCK, GROUPS, per_group), axis=1)
    causal = jnp.tril(jnp.ones((BLOCK, BLOCK), dtype=bool))

    def one_block(carry_state, inputs):
        value_block, in_block, out_block, running_block = inputs
        scores = jnp.einsum('lgn,sgn->gls', out_block, in_block, precision=HIGHEST)
        ordered = jnp.moveaxis(running_block, 0, -1)
        between = jnp.exp(jnp.where(causal, ordered[..., :, None] - ordered[..., None, :], -jnp.inf))
        inside = jnp.einsum('grls,sgrp->lgrp', scores[:, None] * between, value_block, precision=HIGHEST)
        carried = jnp.einsum('lgn,grpn->lgrp', out_block, carry_state, precision=HIGHEST)
        carried = carried * jnp.exp(running_block)[..., None]
        to_end = jnp.exp(running_block[-1][None] - running_block)
        block_states = jnp.einsum('lgn,lgr,lgrp->grpn', in_block, to_end, value_block, precision=HIGHEST)
        next_state = carry_state * jnp.exp(running_block[-1])[..., None, None] + block_states
        return (next_state, inside + carried)
    zero_state = jnp.zeros((GROUPS, per_group, HEADDIM, NSTATE), jnp.float32)
    unused, outputs = lax.scan(one_block, zero_state, (scaled_values, in_blocks, out_blocks, running))
    mixed_out = outputs + head_values * head_direct_gain.reshape(GROUPS, per_group)[:, :, None]
    gated_out = mixed_out.reshape(length, channels) * jax.nn.silu(gate_preactivation.astype(jnp.float32))
    grouped = gated_out.reshape(length, GROUPS, channels // GROUPS)
    normed = grouped * lax.rsqrt(lax.optimization_barrier(jnp.mean(grouped * grouped, axis=-1, keepdims=True)) + EPSILON)
    return (normed.reshape(length, channels) * grouped_norm_gain).astype(jnp.bfloat16)

def routed_reference(second_micro_tokens, expert_norm_gain, routes, visit_weight, gate_weight_table, up_weight_table, down_weight_table):
    tokens, feature_count = second_micro_tokens.shape
    fanout = routes.shape[1]
    experts = gate_weight_table.shape[0]
    values = second_micro_tokens.astype(jnp.float32)
    centered = values - lax.optimization_barrier(jnp.mean(values, axis=1, keepdims=True))
    normed = centered * lax.rsqrt(lax.optimization_barrier(jnp.mean(centered * centered, axis=1, keepdims=True)) + EPSILON)
    normed = (normed * expert_norm_gain).astype(jnp.bfloat16)
    flat_routes = routes.reshape(-1)
    one_hot = (flat_routes[:, None] == jnp.arange(experts, dtype=jnp.int32)[None, :]).astype(jnp.int32)
    slot_index = lax.optimization_barrier(jnp.sum(jnp.cumsum(one_hot, axis=0) * one_hot, axis=1)) - 1
    limit = N_EP * N_TP * CAP
    owners = jnp.arange(tokens * fanout, dtype=jnp.int32) // fanout
    table = jnp.full((experts, limit), tokens, jnp.int32).at[flat_routes, slot_index].set(owners)
    scales = jnp.zeros((experts, limit), jnp.float32).at[flat_routes, slot_index].set(visit_weight.reshape(-1))
    padded = jnp.concatenate([normed, jnp.zeros((1, feature_count), jnp.bfloat16)], axis=0)

    def one_expert(running_sum, inputs):
        row_index, row_scale, gate_piece, up_piece, down_piece = inputs
        routed_rows = padded[row_index]
        activated = jax.nn.silu(jnp.dot(routed_rows, gate_piece, preferred_element_type=jnp.float32))
        hidden = (activated * jnp.dot(routed_rows, up_piece, preferred_element_type=jnp.float32)).astype(jnp.bfloat16)
        result = lax.dot_general(hidden, down_piece, (((1,), (1,)), ((), ())), preferred_element_type=jnp.float32).astype(jnp.bfloat16)
        return (running_sum.at[row_index].add(result.astype(jnp.float32) * row_scale[:, None]), None)
    zero_sum = jnp.zeros((tokens + 1, feature_count), jnp.float32)
    summed_total, unused = lax.scan(one_expert, zero_sum, (table, scales, gate_weight_table, up_weight_table, down_weight_table))
    return summed_total[:tokens].astype(jnp.bfloat16)

def reference(first_micro_values, group_state_maps, gate_preactivation, step_preactivation, head_step_bias, head_log_decay, decay_increment, head_direct_gain, convolution_value_taps, convolution_map_taps, grouped_norm_gain, second_micro_tokens, expert_norm_gain, routes, visit_weight, gate_weight_table, up_weight_table, down_weight_table):
    mixer_gated_output = mixer_baseline(first_micro_values, group_state_maps, gate_preactivation, step_preactivation, head_step_bias, head_log_decay, decay_increment, head_direct_gain, convolution_value_taps, convolution_map_taps, grouped_norm_gain)
    routed_out = routed_reference(second_micro_tokens, expert_norm_gain, routes, visit_weight, gate_weight_table, up_weight_table, down_weight_table)
    return (mixer_gated_output, routed_out)
```

```python
import jax
import jax.numpy as jnp
from jax import lax
from jax.experimental import pallas as pl
from jax.experimental.pallas import tpu as pltpu
from jax.sharding import Mesh
from jax.sharding import PartitionSpec as P

HEADDIM = 64
NSTATE = 128
BLOCK = 128
EP = ("ep_0", "ep_1", "ep_2")
EP_TP = ("ep_0", "ep_1", "ep_2", "tp")


EPSILON = 1e-05
CONTRACT_LAST = (((1,), (1,)), ((), ()))


def shifted(block, axis, distance):
    devices = range(lax.axis_size(axis))
    route = [(i - distance, i) for i in devices if i - distance in devices]
    return lax.ppermute(block, axis, route)


def nothing_yet(x, identity):
    return jax.tree.map(
        lambda part, zero: jnp.zeros_like(part) + jnp.asarray(zero, part.dtype), x, identity
    )


def entering_2(x, axes, combine, identity):
    before = start = nothing_yet(x, identity)
    total = x
    for axis in reversed(axes):
        count, mine = (lax.axis_size(axis), lax.axis_index(axis))
        pieces = jax.tree.map(lambda part: lax.all_gather(part, axis), total)
        inside, total = (start, start)
        for k in range(count):
            passed = k < mine
            total = combine(total, jax.tree.map(lambda part: part[k], pieces))
            inside = jax.tree.map(lambda new, old: jnp.where(passed, new, old), total, inside)
        before = combine(inside, before)
    return before


def causal_conv(before, values, weights):
    length = values.shape[0]
    kernel = weights.shape[0]
    padded = jnp.concatenate([before, values], axis=0).astype(jnp.float32)
    summed_total = jnp.zeros(values.shape, jnp.float32)
    for offset in range(kernel):
        summed_total = (
            summed_total + weights[offset].astype(jnp.float32) * padded[offset : offset + length]
        )
    return jax.nn.silu(summed_total)


def combine_states(earlier, later):
    return (earlier[0] * later[0], earlier[1] * later[0][..., None, None] + later[1])


def mixer_half(
    first_micro_values,
    group_state_maps,
    gate_preactivation,
    step_preactivation,
    head_step_bias,
    head_log_decay,
    decay_increment,
    head_direct_gain,
    convolution_value_taps,
    convolution_map_taps,
    grouped_norm_gain,
):
    length, channels = first_micro_values.shape
    head_count = step_preactivation.shape[1]
    maps_width = group_state_maps.shape[2]
    groups = maps_width // NSTATE
    per_group = head_count // groups
    blocks = length // BLOCK
    conv_reach = convolution_value_taps.shape[0] - 1
    tail_rows = jnp.concatenate(
        [
            first_micro_values[length - conv_reach :],
            group_state_maps[0, length - conv_reach :],
            group_state_maps[1, length - conv_reach :],
        ],
        axis=1,
    )
    before = shifted(tail_rows, EP, 1)
    conv_out = causal_conv(before[:, :channels], first_micro_values, convolution_value_taps)
    in_maps = causal_conv(
        before[:, channels : channels + maps_width], group_state_maps[0], convolution_map_taps[0]
    )
    out_maps = causal_conv(
        before[:, channels + maps_width :], group_state_maps[1], convolution_map_taps[1]
    )
    step_length = jax.nn.softplus(step_preactivation + head_step_bias)
    decay_logarithm = -jnp.exp(head_log_decay) * step_length + decay_increment
    head_values = conv_out.reshape(blocks, BLOCK, groups, per_group, HEADDIM)
    scaled_values = head_values * step_length.reshape(blocks, BLOCK, groups, per_group)[..., None]
    in_blocks = in_maps.reshape(blocks, BLOCK, groups, NSTATE)
    out_blocks = out_maps.reshape(blocks, BLOCK, groups, NSTATE)
    running = jnp.cumsum(decay_logarithm.reshape(blocks, BLOCK, groups, per_group), axis=1)
    causal = jnp.tril(jnp.ones((BLOCK, BLOCK), dtype=bool))
    scores = jnp.einsum("blgn,bsgn->bgls", out_blocks, in_blocks)
    ordered = jnp.moveaxis(running, 1, -1)
    between = jnp.exp(jnp.where(causal, ordered[..., :, None] - ordered[..., None, :], -jnp.inf))
    inside = jnp.einsum("bgrls,bsgrp->blgrp", scores[:, :, None] * between, scaled_values)
    block_total = running[:, -1]
    to_end = jnp.exp(block_total[:, None] - running)
    block_states = jnp.einsum("blgn,blgr,blgrp->bgrpn", in_blocks, to_end, scaled_values)

    def carry_block(carry_state, inputs):
        return (carry_state * jnp.exp(inputs[1])[..., None, None] + inputs[0], carry_state)

    zero_state = jnp.zeros((groups, per_group, HEADDIM, NSTATE), jnp.float32)
    local_end, local_enter = lax.scan(carry_block, zero_state, (block_states, block_total))
    device_decay = jnp.exp(jnp.sum(block_total, axis=0))
    identity = (jnp.ones_like(device_decay), jnp.zeros_like(local_end))
    unused, incoming = entering_2((device_decay, local_end), EP, combine_states, identity)
    prefix = jnp.exp(jnp.cumsum(block_total, axis=0) - block_total)
    entering = local_enter + prefix[..., None, None] * incoming[None]
    carried = jnp.einsum("blgn,bgrpn->blgrp", out_blocks, entering)
    carried = carried * jnp.exp(running)[..., None]
    mixed_out = (
        inside + carried + head_values * head_direct_gain.reshape(groups, per_group)[:, :, None]
    )
    gated_out = mixed_out.reshape(length, channels) * jax.nn.silu(
        gate_preactivation.astype(jnp.float32)
    )
    grouped = gated_out.reshape(length, groups, channels // groups)
    normed = grouped * lax.rsqrt(jnp.mean(grouped * grouped, axis=-1, keepdims=True) + EPSILON)
    return (normed.reshape(length, channels) * grouped_norm_gain).astype(jnp.bfloat16)


SLOTS = 12
ORDER = (4, 1, 7, 3, 5, 2, 6, 0)
MESH_IDS = pl.DeviceIdType.MESH


def here():
    return (lax.axis_index("ep_0"), lax.axis_index("ep_1"), lax.axis_index("ep_2"))


def beside(step):
    return {"tp": lax.rem(lax.axis_index("tp") + step, 4)}


def ep_target(place, dz, dxc):
    z, x, c = place
    tz = lax.rem(z + dz, 8)
    tx = lax.rem(x + lax.div(dxc, 2), 4)
    tc = lax.rem(c + lax.rem(dxc, 2), 2)
    return tz * 8 + tx * 2 + tc, {"ep_0": tz, "ep_1": tx, "ep_2": tc}


def for_all_peers(act):
    place = here()

    def some(dxc, unused):
        for dz in ORDER:
            act(*ep_target(place, dz, dxc))
        return unused

    for dz in ORDER:
        if dz:
            act(*ep_target(place, dz, 0))
    lax.fori_loop(1, 8, some, 0)


def exchange(source, landing, send_sem, recv_sem):
    z, x, c = here()
    me = z * 8 + x * 2 + c

    def send(index, device):
        pltpu.make_async_remote_copy(
            src_ref=source.at[index],
            dst_ref=landing.at[me],
            send_sem=send_sem,
            recv_sem=recv_sem,
            device_id=device,
            device_id_type=MESH_IDS,
        ).start()

    for_all_peers(send)


def all_but_one(source, landing, send_sem, recv_sem):
    return pltpu.make_async_remote_copy(
        src_ref=source.at[pl.ds(0, 63)],
        dst_ref=landing.at[pl.ds(0, 63)],
        send_sem=send_sem,
        recv_sem=recv_sem,
        device_id=beside(1),
        device_id_type=MESH_IDS,
    )


def floor_div(values, divisor):
    return jnp.floor((values + 0.5) * (1.0 / divisor))


def iota(shape, axis):
    return lax.broadcasted_iota(jnp.int32, shape, axis).astype(jnp.float32)


def dot(a, b):
    return jnp.dot(a, b, preferred_element_type=jnp.float32)


def repack_matrix():
    size = 16 * SLOTS
    row = iota((size, size), 0)
    outer = floor_div(row, 4 * SLOTS)
    rest = row - 4 * SLOTS * outer
    inner = floor_div(rest, SLOTS)
    partner = inner * (4 * SLOTS) + outer * SLOTS + (rest - inner * SLOTS)
    return jnp.where(iota((size, size), 1) == partner, 1.0, 0.0).astype(jnp.bfloat16)


def pack_rows(source, landing, matrix, width):
    def group(g, unused):
        rows = source[pl.ds(pl.multiple_of(g * 48, 16), 48), :]
        tall = jnp.concatenate([rows[:, p * width : (p + 1) * width] for p in range(4)], axis=0)
        landing[pl.ds(g * 4, 4)] = dot(matrix, tall).astype(jnp.bfloat16).reshape(4, 48, width)
        return unused

    lax.fori_loop(0, 16, group, 0)


def unpack_rows(source, landing, matrix, width):
    def group(g, unused):
        tall = source[pl.ds(g * 4, 4)].reshape(192, width)
        rows = dot(matrix, tall).astype(jnp.bfloat16)
        for p in range(4):
            landing[pl.ds(pl.multiple_of(g * 48, 16), 48), p * width : (p + 1) * width] = rows[
                p * 48 : (p + 1) * 48
            ]
        return unused

    lax.fori_loop(0, 16, group, 0)


class Neighbours:
    def __init__(self, own, slots, send_sems, recv_sems, first, start, size):
        half = size // 2
        whole, low, high = pl.ds(start, size), pl.ds(start, half), pl.ds(start + half, half)

        def copy(which, source, landing, step):
            return pltpu.make_async_remote_copy(
                src_ref=source,
                dst_ref=landing,
                send_sem=send_sems.at[first + which],
                recv_sem=recv_sems.at[first + which],
                device_id=beside(step),
                device_id_type=MESH_IDS,
            )

        self.near = (
            copy(0, own.at[0, whole], slots.at[1, whole], 1),
            copy(1, own.at[0, whole], slots.at[2, whole], 3),
        )
        self.far = (
            copy(2, slots.at[1, low], slots.at[3, low], 1),
            copy(3, slots.at[2, high], slots.at[3, high], 3),
        )

    def start(self):
        for copy in self.near:
            copy.start()

    def forward(self):
        for arrived, onward in zip(self.near, self.far):
            arrived.wait_recv()
            onward.start()

    def arrive(self):
        for copy in self.far:
            copy.wait_recv()

    def drain(self):
        for copy in self.near + self.far:
            copy.wait_send()


def routed_kernel(
    tokens_hbm,
    gain_ref,
    routes_ref,
    weight_ref,
    gate_hbm,
    up_hbm,
    down_hbm,
    out_ref,
    tokens,
    normed,
    choice,
    mix_high,
    mix_low,
    rows_ref,
    sent,
    landed,
    hidden,
    answers,
    returned,
    gate,
    up,
    down,
    local_sems,
    near_send,
    near_recv,
    dispatch_sems,
    answer_send,
    answer_recv,
):
    own_copies = [
        pltpu.make_async_copy(tokens_hbm, tokens, local_sems.at[0]),
        pltpu.make_async_copy(gate_hbm.at[0], gate.at[0], local_sems.at[1]),
        pltpu.make_async_copy(up_hbm.at[0], up.at[0], local_sems.at[2]),
        pltpu.make_async_copy(down_hbm.at[0], down.at[0], local_sems.at[3]),
    ]
    for copy in own_copies:
        copy.start()
    barrier = pltpu.get_barrier_semaphore()

    def greet(unused, device):
        pl.semaphore_signal(barrier, inc=1, device_id=device, device_id_type=MESH_IDS)

    for step in (1, 3):
        greet(0, beside(step))
    for_all_peers(greet)
    pl.semaphore_wait(barrier, 65)

    gate_near = Neighbours(gate_hbm, gate, near_send, near_recv, 0, 0, 2048)
    up_near = Neighbours(up_hbm, up, near_send, near_recv, 4, 0, 2048)
    down_near = [
        Neighbours(down_hbm, down, near_send, near_recv, 8 + 4 * p, p * 512, 512) for p in range(4)
    ]
    gate_near.start()
    up_near.start()

    own_copies[0].wait()

    def norm_rows(i, unused):
        rows = pl.ds(pl.multiple_of(i * 32, 32), 32)
        values = tokens[rows, :].astype(jnp.float32)
        centered = values - jnp.mean(values, axis=1, keepdims=True)
        scale = lax.rsqrt(jnp.mean(centered * centered, axis=1, keepdims=True) + EPSILON)
        normed[rows, :] = (centered * scale * gain_ref[...]).astype(jnp.bfloat16)
        return unused

    lax.fori_loop(0, 8, norm_rows, 0)

    experts = lax.broadcasted_iota(jnp.int32, (256, 64), 1)
    hits = [jnp.where(routes_ref[:, k : k + 1] == experts, 1.0, 0.0) for k in range(2)]
    named = hits[0] + hits[1]
    earlier = jnp.where(iota((256, 256), 0) > iota((256, 256), 1), 1.0, 0.0).astype(jnp.bfloat16)
    place = dot(earlier, named.astype(jnp.bfloat16))
    key = jnp.where(named > 0.5, place, -1.0)
    key_rows = jnp.transpose(key).astype(jnp.bfloat16)
    slot_rows = iota((768, 64), 0)
    spread = jnp.where(floor_div(slot_rows, SLOTS) == iota((768, 64), 1), 1.0, 0.0)
    spread = spread.astype(jnp.bfloat16)
    wanted = iota((768, 256), 0)
    wanted = wanted - SLOTS * floor_div(wanted, SLOTS)
    choice[...] = jnp.where(dot(spread, key_rows) == wanted, 1.0, 0.0).astype(jnp.bfloat16)
    matrix = repack_matrix()

    def pick(p, unused):
        columns = pl.ds(pl.multiple_of(p * 512, 512), 512)
        rows_ref[:, columns] = dot(choice[...], normed[:, columns]).astype(jnp.bfloat16)
        return unused

    lax.fori_loop(0, 4, pick, 0)
    pack_rows(rows_ref, sent, matrix, 512)
    exchange(sent, landed, dispatch_sems.at[0], dispatch_sems.at[1])
    z, x, c = here()
    me = z * 8 + x * 2 + c
    landed[me] = sent[me]

    weights = weight_ref[:, 0:1] * hits[0] + weight_ref[:, 1:2] * hits[1]
    columns = iota((64, 768), 1)
    spread_columns = jnp.where(floor_div(columns, SLOTS) == iota((64, 768), 0), 1.0, 0.0)
    spread_columns = spread_columns.astype(jnp.bfloat16)
    wanted = iota((256, 768), 1)
    wanted = wanted - SLOTS * floor_div(wanted, SLOTS)
    mine = dot(key.astype(jnp.bfloat16), spread_columns) == wanted
    high = weights.astype(jnp.bfloat16)
    low = (weights - high.astype(jnp.float32)).astype(jnp.bfloat16)
    mix_high[...] = jnp.where(mine, dot(high, spread_columns), 0.0).astype(jnp.bfloat16)
    mix_low[...] = jnp.where(mine, dot(low, spread_columns), 0.0).astype(jnp.bfloat16)

    gate_near.forward()
    up_near.forward()
    for part in down_near:
        part.start()
    gate_near.arrive()
    up_near.arrive()
    for part in down_near:
        part.forward()
    for copy in own_copies[1:]:
        copy.wait()

    all_but_one(sent, landed, dispatch_sems.at[0], dispatch_sems.at[1]).wait()
    unpack_rows(landed, rows_ref, matrix, 512)

    def activate(j, unused):
        for r in range(3):
            rows = rows_ref[r * 256 : (r + 1) * 256, :]
            opened = dot(rows, gate[j])
            raised = dot(rows, up[j])
            hidden[j, r * 256 : (r + 1) * 256, :] = (jax.nn.silu(opened) * raised).astype(
                jnp.bfloat16
            )
        return unused

    lax.fori_loop(0, 4, activate, 0)

    for p in range(4):
        down_near[p].arrive()

        def answer(n, unused):
            lines = pl.ds(pl.multiple_of(p * 512 + n * 256, 256), 256)
            total = jnp.zeros((768, 256), jnp.float32)
            for j in range(4):
                total = total + lax.dot_general(
                    hidden[j], down[j, lines, :], CONTRACT_LAST, preferred_element_type=jnp.float32
                )
            rows_ref[:, lines] = total.astype(jnp.bfloat16)
            return unused

        lax.fori_loop(0, 2, answer, 0)
        pack_rows(rows_ref.at[:, pl.ds(p * 512, 512)], answers.at[p], matrix, 128)
        exchange(answers.at[p], returned.at[p], answer_send.at[p], answer_recv.at[p])
        returned[p, me] = answers[p, me]

    for p in range(4):
        all_but_one(answers.at[p], returned.at[p], answer_send.at[p], answer_recv.at[p]).wait()
        lines = pl.ds(p * 512, 512)
        unpack_rows(returned.at[p], rows_ref.at[:, lines], matrix, 128)
        out_ref[:, lines] = (
            dot(mix_high[...], rows_ref[:, lines]) + dot(mix_low[...], rows_ref[:, lines])
        ).astype(jnp.bfloat16)

    for near in [gate_near, up_near] + down_near:
        near.drain()


def routed_half(
    second_micro_tokens,
    expert_norm_gain,
    routes,
    visit_weight,
    gate_weight_table,
    up_weight_table,
    down_weight_table,
):
    vmem = pl.BlockSpec(memory_space=pltpu.VMEM)
    hbm = pl.BlockSpec(memory_space=pl.ANY)
    bf16 = jnp.bfloat16
    return pl.pallas_call(
        routed_kernel,
        out_shape=jax.ShapeDtypeStruct((256, 2048), bf16),
        in_specs=[hbm, vmem, vmem, vmem, hbm, hbm, hbm],
        out_specs=vmem,
        scratch_shapes=[
            pltpu.VMEM((256, 2048), bf16),
            pltpu.VMEM((256, 2048), bf16),
            pltpu.VMEM((768, 256), bf16),
            pltpu.VMEM((256, 768), bf16),
            pltpu.VMEM((256, 768), bf16),
            pltpu.VMEM((768, 2048), bf16),
            pltpu.VMEM((64, 48, 512), bf16),
            pltpu.VMEM((64, 48, 512), bf16),
            pltpu.VMEM((4, 768, 256), bf16),
            pltpu.VMEM((4, 64, 48, 128), bf16),
            pltpu.VMEM((4, 64, 48, 128), bf16),
            pltpu.VMEM((4, 2048, 256), bf16),
            pltpu.VMEM((4, 2048, 256), bf16),
            pltpu.VMEM((4, 2048, 256), bf16),
            pltpu.SemaphoreType.DMA((4,)),
            pltpu.SemaphoreType.DMA((24,)),
            pltpu.SemaphoreType.DMA((24,)),
            pltpu.SemaphoreType.DMA((2,)),
            pltpu.SemaphoreType.DMA((4,)),
            pltpu.SemaphoreType.DMA((4,)),
        ],
        compiler_params=pltpu.CompilerParams(
            collective_id=0, has_side_effects=True, vmem_limit_bytes=60 * 2**20
        ),
        cost_estimate=pl.CostEstimate(
            flops=10**10, bytes_accessed=2 * 10**7, transcendentals=10**6
        ),
    )(
        second_micro_tokens,
        expert_norm_gain.reshape(1, -1),
        routes,
        visit_weight,
        gate_weight_table,
        up_weight_table,
        down_weight_table,
    )


def body(
    first_micro_values,
    group_state_maps,
    gate_preactivation,
    step_preactivation,
    head_step_bias,
    head_log_decay,
    decay_increment,
    head_direct_gain,
    convolution_value_taps,
    convolution_map_taps,
    grouped_norm_gain,
    second_micro_tokens,
    expert_norm_gain,
    routes,
    visit_weight,
    gate_weight_table,
    up_weight_table,
    down_weight_table,
):
    mixer_gated_output = mixer_half(
        first_micro_values,
        group_state_maps,
        gate_preactivation,
        step_preactivation,
        head_step_bias,
        head_log_decay,
        decay_increment,
        head_direct_gain,
        convolution_value_taps,
        convolution_map_taps,
        grouped_norm_gain,
    )
    routed_out = routed_half(
        second_micro_tokens,
        expert_norm_gain,
        routes,
        visit_weight,
        gate_weight_table,
        up_weight_table,
        down_weight_table,
    )
    return (mixer_gated_output, routed_out)


def solution(mesh):
    torus = Mesh(mesh.devices.reshape(8, 4, 2, mesh.shape["tp"]), ("ep_0", "ep_1", "ep_2", "tp"))
    in_specs = (
        P(EP, "tp"),
        P(None, EP, "tp"),
        P(EP, "tp"),
        P(EP, "tp"),
        P("tp"),
        P("tp"),
        P(EP, "tp"),
        P("tp"),
        P(None, "tp"),
        P(None, None, "tp"),
        P("tp"),
        P(EP_TP, None),
        P(),
        P(EP_TP, None),
        P(EP_TP, None),
        P(EP, None, "tp"),
        P(EP, None, "tp"),
        P(EP, None, "tp"),
    )
    out_specs = (P(EP, "tp"), P(EP_TP, None))
    return jax.shard_map(body, mesh=torus, in_specs=in_specs, out_specs=out_specs, check_vma=False)
```

```python
import types

import jax
import jax.numpy as jnp
from jax import lax
from jax.experimental import pallas as pl
from jax.experimental.pallas import tpu as pltpu
from jax.sharding import Mesh
from jax.sharding import PartitionSpec as P

HEADDIM = 64
NSTATE = 128
BLOCK = 128
SEQ_BLOCKS = 8
EP = ("ep_0", "ep_1", "ep_2")
EP_TP = ("ep_0", "ep_1", "ep_2", "tp")


EPSILON = 1e-05
CONTRACT_LAST = (((1,), (1,)), ((), ()))


SLOTS = 12
ORDER = (4, 1, 7, 3, 5, 2, 6, 0)
MESH_IDS = pl.DeviceIdType.MESH


def here():
    return (lax.axis_index("ep_0"), lax.axis_index("ep_1"), lax.axis_index("ep_2"))


def beside(step):
    return {"tp": lax.rem(lax.axis_index("tp") + step, 4)}


def ep_target(place, dz, dxc):
    z, x, c = place
    tz = lax.rem(z + dz, 8)
    tx = lax.rem(x + lax.div(dxc, 2), 4)
    tc = lax.rem(c + lax.rem(dxc, 2), 2)
    return tz * 8 + tx * 2 + tc, {"ep_0": tz, "ep_1": tx, "ep_2": tc}


def for_all_peers(act):
    place = here()

    def some(dxc, unused):
        for dz in ORDER:
            act(*ep_target(place, dz, dxc))
        return unused

    for dz in ORDER:
        if dz:
            act(*ep_target(place, dz, 0))
    lax.fori_loop(1, 8, some, 0)


def exchange(source, landing, send_sem, recv_sem):
    z, x, c = here()
    me = z * 8 + x * 2 + c

    def send(index, device):
        pltpu.make_async_remote_copy(
            src_ref=source.at[index],
            dst_ref=landing.at[me],
            send_sem=send_sem,
            recv_sem=recv_sem,
            device_id=device,
            device_id_type=MESH_IDS,
        ).start()

    for_all_peers(send)


def all_but_one(source, landing, send_sem, recv_sem):
    return pltpu.make_async_remote_copy(
        src_ref=source.at[pl.ds(0, 63)],
        dst_ref=landing.at[pl.ds(0, 63)],
        send_sem=send_sem,
        recv_sem=recv_sem,
        device_id=beside(1),
        device_id_type=MESH_IDS,
    )


def floor_div(values, divisor):
    return jnp.floor((values + 0.5) * (1.0 / divisor))


def iota(shape, axis):
    return lax.broadcasted_iota(jnp.int32, shape, axis).astype(jnp.float32)


def dot(a, b):
    return jnp.dot(a, b, preferred_element_type=jnp.float32)


def repack_matrix():
    size = 16 * SLOTS
    row = iota((size, size), 0)
    outer = floor_div(row, 4 * SLOTS)
    rest = row - 4 * SLOTS * outer
    inner = floor_div(rest, SLOTS)
    partner = inner * (4 * SLOTS) + outer * SLOTS + (rest - inner * SLOTS)
    return jnp.where(iota((size, size), 1) == partner, 1.0, 0.0).astype(jnp.bfloat16)


def pack_rows(source, landing, matrix, width):
    def group(g, unused):
        rows = source[pl.ds(pl.multiple_of(g * 48, 16), 48), :]
        tall = jnp.concatenate([rows[:, p * width : (p + 1) * width] for p in range(4)], axis=0)
        landing[pl.ds(g * 4, 4)] = dot(matrix, tall).astype(jnp.bfloat16).reshape(4, 48, width)
        return unused

    lax.fori_loop(0, 16, group, 0)


def unpack_rows(source, landing, matrix, width):
    def group(g, unused):
        tall = source[pl.ds(g * 4, 4)].reshape(192, width)
        rows = dot(matrix, tall).astype(jnp.bfloat16)
        for p in range(4):
            landing[pl.ds(pl.multiple_of(g * 48, 16), 48), p * width : (p + 1) * width] = rows[
                p * 48 : (p + 1) * 48
            ]
        return unused

    lax.fori_loop(0, 16, group, 0)


class Neighbours:
    def __init__(self, own, slots, send_sems, recv_sems, first, start, size):
        half = size // 2
        whole, low, high = pl.ds(start, size), pl.ds(start, half), pl.ds(start + half, half)

        def copy(which, source, landing, step):
            return pltpu.make_async_remote_copy(
                src_ref=source,
                dst_ref=landing,
                send_sem=send_sems.at[first + which],
                recv_sem=recv_sems.at[first + which],
                device_id=beside(step),
                device_id_type=MESH_IDS,
            )

        self.near = (
            copy(0, own.at[0, whole], slots.at[1, whole], 1),
            copy(1, own.at[0, whole], slots.at[2, whole], 3),
        )
        self.far = (
            copy(2, slots.at[1, low], slots.at[3, low], 1),
            copy(3, slots.at[2, high], slots.at[3, high], 3),
        )

    def start(self):
        for copy in self.near:
            copy.start()

    def forward(self):
        for arrived, onward in zip(self.near, self.far):
            arrived.wait_recv()
            onward.start()

    def arrive(self):
        for copy in self.far:
            copy.wait_recv()

    def drain(self):
        for copy in self.near + self.far:
            copy.wait_send()


def exact_dot(a, b):
    return jnp.dot(a, b, precision=lax.Precision.HIGHEST, preferred_element_type=jnp.float32)


def softplus(values):
    small = jnp.exp(-jnp.abs(values))
    ratio = small / (2.0 + small)
    square = ratio * ratio
    series = 1.0 / 13.0
    for odd in (11.0, 9.0, 7.0, 5.0, 3.0, 1.0):
        series = series * square + 1.0 / odd
    return jnp.maximum(values, 0.0) + 2.0 * ratio * series


def head_spread(rows):
    return jnp.where(floor_div(iota((rows, 512), 1), HEADDIM) == iota((rows, 512), 0), 1.0, 0.0)


def conv_silu(window, taps):
    window = window.astype(jnp.float32)
    total = taps[3:4] * window[16:]
    for j in range(3):
        total = total + taps[j : j + 1] * pltpu.roll(window, 3 - j, 0)[16:]
    return jax.nn.silu(total)


def mixer_local(m):
    spread = head_spread(8)
    low = iota((BLOCK, BLOCK), 0)
    high = iota((BLOCK, BLOCK), 1)
    causal = low >= high
    lower = jnp.where(causal, 1.0, 0.0)
    first = iota((BLOCK, 512), 1)
    first = first - 128 * floor_div(first, 128) < 64
    gain = exact_dot(jnp.broadcast_to(m.direct_gain[...], (8, 8)), spread)[0:1]
    rate = -jnp.exp(m.log_decay[...])
    value_taps = m.value_taps[...].astype(jnp.float32)
    map_taps = m.map_taps[...].astype(jnp.float32)
    m.state[...] = jnp.zeros_like(m.state)

    def block(b, prefix):
        start = pl.multiple_of(b * BLOCK, BLOCK)
        rows, window = pl.ds(start, BLOCK), pl.ds(start, BLOCK + 16)
        x = conv_silu(m.values[window, :], value_taps)
        in_maps = conv_silu(m.maps[0, window, :], map_taps[0])
        out_maps = conv_silu(m.maps[1, window, :], map_taps[1]).astype(jnp.bfloat16)
        m.out_maps[rows, :] = out_maps
        step = softplus(m.step[rows, :] + m.step_bias[...])
        running = exact_dot(lower, rate * step + m.increment[rows, :])
        running_rows = jnp.transpose(running)
        total = running[BLOCK - 1 : BLOCK, :]
        m.decay[rows, :] = jnp.exp(prefix + running)
        scaled = x * exact_dot(step, spread)
        to_end = (x * exact_dot(step * jnp.exp(total - running), spread)).astype(jnp.bfloat16)
        entered = exact_dot(jnp.exp(running), spread)
        left = jnp.where(first, scaled, 0.0).astype(jnp.bfloat16)
        right = jnp.where(first, 0.0, scaled).astype(jnp.bfloat16)
        for g in range(2):
            maps = slice(g * NSTATE, (g + 1) * NSTATE)
            wide = slice(g * 256, (g + 1) * 256)
            scores = lax.dot_general(
                out_maps[:, maps],
                in_maps[:, maps].astype(jnp.bfloat16),
                CONTRACT_LAST,
                preferred_element_type=jnp.float32,
            )
            carried = dot(out_maps[:, maps], m.state[:, wide].astype(jnp.bfloat16))
            for pair in range(2):
                mixes = []
                for h in (g * 4 + 2 * pair, g * 4 + 2 * pair + 1):
                    ahead = running[:, h : h + 1] - running_rows[h : h + 1, :]
                    between = jnp.exp(jnp.where(causal, ahead, -jnp.inf))
                    mixes.append((scores * between).astype(jnp.bfloat16))
                part = slice((g * 2 + pair) * 128, (g * 2 + pair + 1) * 128)
                inside = dot(
                    jnp.concatenate(mixes, axis=1),
                    jnp.concatenate([left[:, part], right[:, part]], axis=0),
                )
                m.mixed[rows, part] = (
                    inside
                    + carried[:, pair * 128 : (pair + 1) * 128] * entered[:, part]
                    + x[:, part] * gain[:, part]
                )
            turned = jnp.transpose(in_maps[:, maps]).astype(jnp.bfloat16)
            m.state[:, wide] = m.state[:, wide] * entered[BLOCK - 1 : BLOCK, wide] + dot(
                turned, to_end[:, wide]
            )
        return prefix + total

    prefix = lax.fori_loop(0, SEQ_BLOCKS, block, jnp.zeros((1, 8), jnp.float32))
    for j in range(8):
        m.state_out[j] = m.state[j * 16 : (j + 1) * 16, :].astype(jnp.bfloat16)
    heads = jnp.where(iota((8, 128), 0) == iota((8, 128), 1), 1.0, 0.0)
    m.decay_out[...] = exact_dot(jnp.broadcast_to(jnp.exp(prefix), (8, 8)), heads)


def plane_target(dxc):
    z, x, c = here()
    tx = lax.rem(x + lax.div(dxc, 2), 4)
    tc = lax.rem(c + lax.rem(dxc, 2), 2)
    return tx * 2 + tc, {"ep_1": tx, "ep_2": tc}


def plane_send(source, landing, send_sem, recv_sem, indexed):
    z, x, c = here()
    mine = x * 2 + c

    def send(dxc, unused):
        index, device = plane_target(dxc)
        pltpu.make_async_remote_copy(
            src_ref=source.at[index] if indexed else source,
            dst_ref=landing.at[mine],
            send_sem=send_sem,
            recv_sem=recv_sem,
            device_id=device,
            device_id_type=MESH_IDS,
        ).start()
        return unused

    lax.fori_loop(1, 8, send, 0)


def plane_wait(landing, send_sem, recv_sem):
    pltpu.make_async_remote_copy(
        src_ref=landing.at[pl.ds(0, 7)],
        dst_ref=landing.at[pl.ds(0, 7)],
        send_sem=send_sem,
        recv_sem=recv_sem,
        device_id=beside(1),
        device_id_type=MESH_IDS,
    ).wait()


def later_copy(m, d, which):
    source, landing = ((m.plane_state, m.early_state), (m.plane_decay, m.early_decay))[which]
    return pltpu.make_async_remote_copy(
        src_ref=source,
        dst_ref=landing.at[d - 1],
        send_sem=m.later_send.at[which, d - 1],
        recv_sem=m.later_recv.at[which, d - 1],
        device_id={"ep_0": lax.rem(lax.axis_index("ep_0") + d, 8)},
        device_id_type=MESH_IDS,
    )


def states_first(m):
    z, x, c = here()
    mine = x * 2 + c
    m.plane_states[mine] = m.state_out[mine]
    m.plane_decays[mine] = m.decay_out[...]
    plane_send(m.state_out, m.plane_states, m.plane_sems.at[0], m.plane_sems.at[1], True)
    plane_send(m.decay_out, m.plane_decays, m.plane_sems.at[2], m.plane_sems.at[3], False)


def states_second(m):
    plane_wait(m.plane_states, m.plane_sems.at[0], m.plane_sems.at[1])
    plane_wait(m.plane_decays, m.plane_sems.at[2], m.plane_sems.at[3])
    spread = head_spread(128)
    before = jnp.zeros((16, 512), jnp.float32)
    passed = jnp.ones((8, 128), jnp.float32)
    for j in range(8):
        m.before[j] = before
        m.passed[j] = passed
        decay = m.plane_decays[j]
        before = before * exact_dot(decay, spread)[0:1] + m.plane_states[j].astype(jnp.float32)
        passed = passed * decay
    m.plane_state[...] = before.astype(jnp.bfloat16)
    m.plane_decay[...] = passed
    z = lax.axis_index("ep_0")
    for d in range(1, 8):

        @pl.when(z + d < 8)
        def _():
            for which in range(2):
                later_copy(m, d, which).start()


def states_third(m):
    z, x, c = here()
    spread = head_spread(128)
    m.incoming[...] = jnp.zeros_like(m.incoming)
    for d in range(7, 0, -1):

        @pl.when(z >= d)
        def _():
            for which in range(2):
                later_copy(m, d, which).wait_recv()
            m.incoming[...] = m.incoming[...] * exact_dot(m.early_decay[d - 1], spread)[
                0:1
            ] + m.early_state[d - 1].astype(jnp.float32)

    incoming = m.incoming[...]
    for j in range(8):
        entering = m.before[j] + exact_dot(m.passed[j], spread)[0:1] * incoming
        m.answer_states[j] = entering.astype(jnp.bfloat16)
    mine = x * 2 + c
    m.entering[mine] = m.answer_states[mine]
    plane_send(m.answer_states, m.entering, m.plane_sems.at[4], m.plane_sems.at[5], True)
    for d in range(1, 8):

        @pl.when(z + d < 8)
        def _():
            for which in range(2):
                later_copy(m, d, which).wait_send()


def mixer_finish(m):
    plane_wait(m.entering, m.plane_sems.at[4], m.plane_sems.at[5])
    spread = head_spread(8)
    entering = m.entering[...].reshape(128, 512)

    def block(b, unused):
        rows = pl.ds(pl.multiple_of(b * BLOCK, BLOCK), BLOCK)
        decay = exact_dot(m.decay[rows, :], spread)
        for g in range(2):
            wide = slice(g * 256, (g + 1) * 256)
            carried = dot(m.out_maps[rows, g * NSTATE : (g + 1) * NSTATE], entering[:, wide])
            gated = (m.mixed[rows, wide] + carried * decay[:, wide]) * jax.nn.silu(
                m.gate[rows, wide].astype(jnp.float32)
            )
            scale = lax.rsqrt(jnp.mean(gated * gated, axis=1, keepdims=True) + EPSILON)
            m.result[rows, wide] = (gated * scale * m.norm_gain[:, wide]).astype(jnp.bfloat16)
        return unused

    lax.fori_loop(0, SEQ_BLOCKS, block, 0)


BF16 = jnp.bfloat16
F32 = jnp.float32

INPUTS = (
    "tokens_hbm",
    "expert_gain",
    "routes",
    "visit_weight",
    "gate_hbm",
    "up_hbm",
    "down_hbm",
    "values_hbm",
    "maps_hbm",
    "gate_pre_hbm",
    "step_hbm",
    "increment_hbm",
    "step_bias",
    "log_decay",
    "direct_gain",
    "value_taps",
    "map_taps",
    "norm_gain",
)
OUTPUTS = ("result", "routed_out")
SCRATCH = dict(
    tokens=pltpu.VMEM((256, 2048), BF16),
    normed=pltpu.VMEM((256, 2048), BF16),
    choice=pltpu.VMEM((768, 256), BF16),
    mix_high=pltpu.VMEM((256, 768), BF16),
    mix_low=pltpu.VMEM((256, 768), BF16),
    rows=pltpu.VMEM((768, 2048), BF16),
    sent=pltpu.VMEM((64, 48, 512), BF16),
    landed=pltpu.VMEM((64, 48, 512), BF16),
    hidden=pltpu.VMEM((4, 768, 256), BF16),
    answers=pltpu.VMEM((4, 64, 48, 128), BF16),
    returned=pltpu.VMEM((4, 64, 48, 128), BF16),
    gate_slots=pltpu.VMEM((4, 2048, 256), BF16),
    up_slots=pltpu.VMEM((4, 2048, 256), BF16),
    down_slots=pltpu.VMEM((4, 2048, 256), BF16),
    values=pltpu.VMEM((1040, 512), BF16),
    maps=pltpu.VMEM((2, 1040, 256), BF16),
    gate=pltpu.VMEM((1024, 512), BF16),
    step=pltpu.VMEM((1024, 8), F32),
    increment=pltpu.VMEM((1024, 8), F32),
    decay=pltpu.VMEM((1024, 8), F32),
    mixed=pltpu.VMEM((1024, 512), F32),
    out_maps=pltpu.VMEM((1024, 256), BF16),
    state=pltpu.VMEM((128, 512), F32),
    state_out=pltpu.VMEM((8, 16, 512), BF16),
    decay_out=pltpu.VMEM((8, 128), F32),
    plane_states=pltpu.VMEM((8, 16, 512), BF16),
    plane_decays=pltpu.VMEM((8, 8, 128), F32),
    before=pltpu.VMEM((8, 16, 512), F32),
    passed=pltpu.VMEM((8, 8, 128), F32),
    plane_state=pltpu.VMEM((16, 512), BF16),
    plane_decay=pltpu.VMEM((8, 128), F32),
    early_state=pltpu.VMEM((7, 16, 512), BF16),
    early_decay=pltpu.VMEM((7, 8, 128), F32),
    incoming=pltpu.VMEM((16, 512), F32),
    answer_states=pltpu.VMEM((8, 16, 512), BF16),
    entering=pltpu.VMEM((8, 16, 512), BF16),
    local_sems=pltpu.SemaphoreType.DMA((9,)),
    near_send=pltpu.SemaphoreType.DMA((24,)),
    near_recv=pltpu.SemaphoreType.DMA((24,)),
    dispatch_sems=pltpu.SemaphoreType.DMA((2,)),
    answer_send=pltpu.SemaphoreType.DMA((4,)),
    answer_recv=pltpu.SemaphoreType.DMA((4,)),
    tail_send=pltpu.SemaphoreType.DMA((2,)),
    tail_recv=pltpu.SemaphoreType.DMA((2,)),
    plane_sems=pltpu.SemaphoreType.DMA((6,)),
    later_send=pltpu.SemaphoreType.DMA((2, 7)),
    later_recv=pltpu.SemaphoreType.DMA((2, 7)),
)


def kernel(*refs):
    m = types.SimpleNamespace(**dict(zip(INPUTS + OUTPUTS + tuple(SCRATCH), refs)))
    place = here()
    z, x, c = place
    me = z * 8 + x * 2 + c
    body = pl.ds(16, 1024)
    own_copies = [
        pltpu.make_async_copy(source, target, m.local_sems.at[i])
        for i, (source, target) in enumerate(
            (
                (m.tokens_hbm, m.tokens),
                (m.values_hbm, m.values.at[body]),
                (m.maps_hbm, m.maps.at[:, body]),
                (m.step_hbm, m.step),
                (m.increment_hbm, m.increment),
                (m.gate_pre_hbm, m.gate),
                (m.gate_hbm.at[0], m.gate_slots.at[0]),
                (m.up_hbm.at[0], m.up_slots.at[0]),
                (m.down_hbm.at[0], m.down_slots.at[0]),
            )
        )
    ]
    for copy in own_copies:
        copy.start()
    barrier = pltpu.get_barrier_semaphore()

    def greet(unused, device):
        pl.semaphore_signal(barrier, inc=1, device_id=device, device_id_type=MESH_IDS)

    for step in (1, 3):
        greet(0, beside(step))
    for_all_peers(greet)
    pl.semaphore_wait(barrier, 65)

    gate_near = Neighbours(m.gate_hbm, m.gate_slots, m.near_send, m.near_recv, 0, 0, 2048)
    up_near = Neighbours(m.up_hbm, m.up_slots, m.near_send, m.near_recv, 4, 0, 2048)
    down_near = [
        Neighbours(m.down_hbm, m.down_slots, m.near_send, m.near_recv, 8 + 4 * p, p * 512, 512)
        for p in range(4)
    ]
    gate_near.start()
    up_near.start()
    down_near[0].start()
    after = lax.rem(me + 1, 64)
    tails = [
        pltpu.make_async_remote_copy(
            src_ref=source,
            dst_ref=target,
            send_sem=m.tail_send.at[i],
            recv_sem=m.tail_recv.at[i],
            device_id={
                "ep_0": lax.div(after, 8),
                "ep_1": lax.rem(lax.div(after, 2), 4),
                "ep_2": lax.rem(after, 2),
            },
            device_id_type=MESH_IDS,
        )
        for i, (source, target) in enumerate(
            (
                (m.values_hbm.at[pl.ds(1008, 16)], m.values.at[pl.ds(0, 16)]),
                (m.maps_hbm.at[:, pl.ds(1008, 16)], m.maps.at[:, pl.ds(0, 16)]),
            )
        )
    ]
    for copy in tails:
        copy.start()

    own_copies[0].wait()

    def norm_rows(i, unused):
        rows = pl.ds(pl.multiple_of(i * 32, 32), 32)
        values = m.tokens[rows, :].astype(jnp.float32)
        centered = values - jnp.mean(values, axis=1, keepdims=True)
        scale = lax.rsqrt(jnp.mean(centered * centered, axis=1, keepdims=True) + EPSILON)
        m.normed[rows, :] = (centered * scale * m.expert_gain[...]).astype(jnp.bfloat16)
        return unused

    lax.fori_loop(0, 8, norm_rows, 0)

    experts = lax.broadcasted_iota(jnp.int32, (256, 64), 1)
    hits = [jnp.where(m.routes[:, k : k + 1] == experts, 1.0, 0.0) for k in range(2)]
    named = hits[0] + hits[1]
    earlier = jnp.where(iota((256, 256), 0) > iota((256, 256), 1), 1.0, 0.0).astype(jnp.bfloat16)
    slot = dot(earlier, named.astype(jnp.bfloat16))
    key = jnp.where(named > 0.5, slot, -1.0)
    key_rows = jnp.transpose(key).astype(jnp.bfloat16)
    spread = jnp.where(
        floor_div(iota((768, 64), 0), SLOTS) == iota((768, 64), 1), 1.0, 0.0
    ).astype(jnp.bfloat16)
    wanted = iota((768, 256), 0)
    wanted = wanted - SLOTS * floor_div(wanted, SLOTS)
    m.choice[...] = jnp.where(dot(spread, key_rows) == wanted, 1.0, 0.0).astype(jnp.bfloat16)
    matrix = repack_matrix()

    def pick(p, unused):
        columns = pl.ds(pl.multiple_of(p * 512, 512), 512)
        m.rows[:, columns] = dot(m.choice[...], m.normed[:, columns]).astype(jnp.bfloat16)
        return unused

    lax.fori_loop(0, 4, pick, 0)
    pack_rows(m.rows, m.sent, matrix, 512)
    exchange(m.sent, m.landed, m.dispatch_sems.at[0], m.dispatch_sems.at[1])
    m.landed[me] = m.sent[me]

    for copy in own_copies[1:5]:
        copy.wait()
    for copy in tails:
        copy.wait_recv()
    m.values[0:16, :] = jnp.where(me > 0, m.values[0:16, :], jnp.zeros((16, 512), jnp.bfloat16))
    m.maps[:, 0:16, :] = jnp.where(me > 0, m.maps[:, 0:16, :], jnp.zeros((2, 16, 256), jnp.bfloat16))
    mixer_local(m)
    gate_near.forward()
    states_first(m)

    weights = m.visit_weight[:, 0:1] * hits[0] + m.visit_weight[:, 1:2] * hits[1]
    spread_columns = jnp.where(
        floor_div(iota((64, 768), 1), SLOTS) == iota((64, 768), 0), 1.0, 0.0
    ).astype(jnp.bfloat16)
    wanted = iota((256, 768), 1)
    wanted = wanted - SLOTS * floor_div(wanted, SLOTS)
    mine = dot(key.astype(jnp.bfloat16), spread_columns) == wanted
    high = weights.astype(jnp.bfloat16)
    low = (weights - high.astype(jnp.float32)).astype(jnp.bfloat16)
    m.mix_high[...] = jnp.where(mine, dot(high, spread_columns), 0.0).astype(jnp.bfloat16)
    m.mix_low[...] = jnp.where(mine, dot(low, spread_columns), 0.0).astype(jnp.bfloat16)

    states_second(m)
    states_third(m)
    up_near.forward()
    down_near[0].forward()
    down_near[1].start()
    down_near[2].start()
    for copy in own_copies[5:]:
        copy.wait()
    mixer_finish(m)
    gate_near.arrive()
    up_near.arrive()

    all_but_one(m.sent, m.landed, m.dispatch_sems.at[0], m.dispatch_sems.at[1]).wait()
    unpack_rows(m.landed, m.rows, matrix, 512)

    def activate(j, unused):
        for r in range(3):
            rows = m.rows[r * 256 : (r + 1) * 256, :]
            opened = dot(rows, m.gate_slots[j])
            raised = dot(rows, m.up_slots[j])
            m.hidden[j, r * 256 : (r + 1) * 256, :] = (jax.nn.silu(opened) * raised).astype(
                jnp.bfloat16
            )
        return unused

    lax.fori_loop(0, 4, activate, 0)

    for p in range(4):
        down_near[p].arrive()

        def answer(n, unused):
            lines = pl.ds(pl.multiple_of(p * 512 + n * 256, 256), 256)
            total = jnp.zeros((768, 256), jnp.float32)
            for j in range(4):
                total = total + lax.dot_general(
                    m.hidden[j],
                    m.down_slots[j, lines, :],
                    CONTRACT_LAST,
                    preferred_element_type=jnp.float32,
                )
            m.rows[:, lines] = total.astype(jnp.bfloat16)
            return unused

        lax.fori_loop(0, 2, answer, 0)
        pack_rows(m.rows.at[:, pl.ds(p * 512, 512)], m.answers.at[p], matrix, 128)
        exchange(m.answers.at[p], m.returned.at[p], m.answer_send.at[p], m.answer_recv.at[p])
        m.returned[p, me] = m.answers[p, me]
        if p < 3:
            down_near[p + 1].forward()
        if p == 0:
            down_near[3].start()

    for p in range(4):
        all_but_one(
            m.answers.at[p], m.returned.at[p], m.answer_send.at[p], m.answer_recv.at[p]
        ).wait()
        lines = pl.ds(p * 512, 512)
        unpack_rows(m.returned.at[p], m.rows.at[:, lines], matrix, 128)
        m.routed_out[:, lines] = (
            dot(m.mix_high[...], m.rows[:, lines]) + dot(m.mix_low[...], m.rows[:, lines])
        ).astype(jnp.bfloat16)

    for near in [gate_near, up_near] + down_near:
        near.drain()
    for copy in tails:
        copy.wait_send()


def body(
    first_micro_values,
    group_state_maps,
    gate_preactivation,
    step_preactivation,
    head_step_bias,
    head_log_decay,
    decay_increment,
    head_direct_gain,
    convolution_value_taps,
    convolution_map_taps,
    grouped_norm_gain,
    second_micro_tokens,
    expert_norm_gain,
    routes,
    visit_weight,
    gate_weight_table,
    up_weight_table,
    down_weight_table,
):
    operands = (
        second_micro_tokens,
        expert_norm_gain.reshape(1, -1),
        routes,
        visit_weight,
        gate_weight_table,
        up_weight_table,
        down_weight_table,
        first_micro_values,
        group_state_maps,
        gate_preactivation,
        step_preactivation,
        decay_increment,
        head_step_bias.reshape(1, -1),
        head_log_decay.reshape(1, -1),
        head_direct_gain.reshape(1, -1),
        convolution_value_taps,
        convolution_map_taps,
        grouped_norm_gain.reshape(1, -1),
    )
    vmem = pl.BlockSpec(memory_space=pltpu.VMEM)
    hbm = pl.BlockSpec(memory_space=pl.ANY)
    return pl.pallas_call(
        kernel,
        out_shape=(
            jax.ShapeDtypeStruct((1024, 512), BF16),
            jax.ShapeDtypeStruct((256, 2048), BF16),
        ),
        in_specs=[hbm if name.endswith("_hbm") else vmem for name in INPUTS],
        out_specs=(vmem, vmem),
        scratch_shapes=list(SCRATCH.values()),
        compiler_params=pltpu.CompilerParams(
            collective_id=0, has_side_effects=True, vmem_limit_bytes=60 * 2**20
        ),
    )(*operands)


def solution(mesh):
    torus = Mesh(mesh.devices.reshape(8, 4, 2, mesh.shape["tp"]), ("ep_0", "ep_1", "ep_2", "tp"))
    in_specs = (
        P(EP, "tp"),
        P(None, EP, "tp"),
        P(EP, "tp"),
        P(EP, "tp"),
        P("tp"),
        P("tp"),
        P(EP, "tp"),
        P("tp"),
        P(None, "tp"),
        P(None, None, "tp"),
        P("tp"),
        P(EP_TP, None),
        P(),
        P(EP_TP, None),
        P(EP_TP, None),
        P(EP, None, "tp"),
        P(EP, None, "tp"),
        P(EP, None, "tp"),
    )
    out_specs = (P(EP, "tp"), P(EP_TP, None))
    return jax.shard_map(body, mesh=torus, in_specs=in_specs, out_specs=out_specs, check_vma=False)
```

```python
import types

import jax
import jax.numpy as jnp
from jax import lax
from jax.experimental import pallas as pl
from jax.experimental.pallas import tpu as pltpu
from jax.sharding import Mesh
from jax.sharding import PartitionSpec as P

HEADDIM = 64
NSTATE = 128
BLOCK = 128
SEQ_BLOCKS = 8
EP = ("ep_0", "ep_1", "ep_2")
EP_TP = ("ep_0", "ep_1", "ep_2", "tp")


EPSILON = 1e-05
CONTRACT_LAST = (((1,), (1,)), ((), ()))


SLOTS = 12
ORDER = (4, 1, 7, 3, 5, 2, 6, 0)
MESH_IDS = pl.DeviceIdType.MESH


def here():
    return (lax.axis_index("ep_0"), lax.axis_index("ep_1"), lax.axis_index("ep_2"))


def beside(step):
    return {"tp": lax.rem(lax.axis_index("tp") + step, 4)}


def around(place, dz, dxc, sign):
    z, x, c = place
    return {
        "ep_0": lax.rem(z + (dz if sign > 0 else 8 - dz), 8),
        "ep_1": lax.rem(x + (lax.div(dxc, 2) if sign > 0 else 4 - lax.div(dxc, 2)), 4),
        "ep_2": lax.rem(c + lax.rem(dxc, 2), 2),
    }


def for_peers(dxc, act, sign):
    place = here()
    for i, dz in enumerate(ORDER):
        act(i, around(place, dz, dxc, sign))


def for_all_peers(act):
    place = here()
    for i, dz in enumerate(ORDER[:7]):
        act(i, around(place, dz, 0, 1))

    def some(dxc, unused):
        for_peers(dxc, lambda i, device: act(dxc * 8 + i, device), 1)
        return unused

    lax.fori_loop(1, 8, some, 0)


def row_copy(source, landing, index, send_sem, recv_sem, device):
    return pltpu.make_async_remote_copy(
        src_ref=source.at[index],
        dst_ref=landing.at[index],
        send_sem=send_sem,
        recv_sem=recv_sem,
        device_id=device,
        device_id_type=MESH_IDS,
    )


def send_group(source, landing, dxc, send_sem, recv_sem, sign):
    place = here()
    first = isinstance(dxc, int) and dxc == 0
    for i, dz in enumerate(ORDER[:7] if first else ORDER):
        device = around(place, dz, dxc, sign)
        row_copy(source, landing, dxc * 8 + i, send_sem, recv_sem, device).start()


def half_bytes(source, landing, half, send_sem, recv_sem):
    rows = pl.ds(0, 31) if half == 0 else pl.ds(32, 32)
    return pltpu.make_async_remote_copy(
        src_ref=source.at[rows],
        dst_ref=landing.at[rows],
        send_sem=send_sem,
        recv_sem=recv_sem,
        device_id=beside(1),
        device_id_type=MESH_IDS,
    )


def floor_div(values, divisor):
    return jnp.floor((values + 0.5) * (1.0 / divisor))


def iota(shape, axis):
    return lax.broadcasted_iota(jnp.int32, shape, axis).astype(jnp.float32)


def dot(a, b):
    return jnp.dot(a, b, preferred_element_type=jnp.float32)


def repack_matrix():
    size = 16 * SLOTS
    row = iota((size, size), 0)
    outer = floor_div(row, 4 * SLOTS)
    rest = row - 4 * SLOTS * outer
    inner = floor_div(rest, SLOTS)
    partner = inner * (4 * SLOTS) + outer * SLOTS + (rest - inner * SLOTS)
    return jnp.where(iota((size, size), 1) == partner, 1.0, 0.0).astype(jnp.bfloat16)


def pack_group(rows, matrix, width):
    tall = jnp.concatenate([rows[:, p * width : (p + 1) * width] for p in range(4)], axis=0)
    return dot(matrix, tall).astype(jnp.bfloat16).reshape(4, 48, width)


def unpack_half(source, landing, matrix, half, column, width):
    for g in range(half * 8, half * 8 + 8):
        rows = dot(matrix, source[g * 4 : g * 4 + 4].reshape(192, width)).astype(jnp.bfloat16)
        for p in range(4):
            landing[g * 48 : (g + 1) * 48, column + p * width : column + (p + 1) * width] = rows[
                p * 48 : (p + 1) * 48
            ]


class Neighbours:
    def __init__(self, own, slots, send_sems, recv_sems, first, start, size):
        half = size // 2
        whole, low, high = pl.ds(start, size), pl.ds(start, half), pl.ds(start + half, half)

        def copy(which, source, landing, step):
            return pltpu.make_async_remote_copy(
                src_ref=source,
                dst_ref=landing,
                send_sem=send_sems.at[first + which],
                recv_sem=recv_sems.at[first + which],
                device_id=beside(step),
                device_id_type=MESH_IDS,
            )

        self.near = (
            copy(0, own.at[0, whole], slots.at[1, whole], 1),
            copy(1, own.at[0, whole], slots.at[2, whole], 3),
        )
        self.far = (
            copy(2, slots.at[1, low], slots.at[3, low], 1),
            copy(3, slots.at[2, high], slots.at[3, high], 3),
        )

    def start(self):
        for copy in self.near:
            copy.start()

    def forward(self):
        for arrived, onward in zip(self.near, self.far):
            arrived.wait_recv()
            onward.start()

    def arrive(self):
        for copy in self.far:
            copy.wait_recv()

    def drain(self):
        for copy in self.near + self.far:
            copy.wait_send()


def exact_dot(a, b):
    return jnp.dot(a, b, precision=lax.Precision.HIGHEST, preferred_element_type=jnp.float32)


def softplus(values):
    small = jnp.exp(-jnp.abs(values))
    ratio = small / (2.0 + small)
    square = ratio * ratio
    series = 1.0 / 13.0
    for odd in (11.0, 9.0, 7.0, 5.0, 3.0, 1.0):
        series = series * square + 1.0 / odd
    return jnp.maximum(values, 0.0) + 2.0 * ratio * series


def head_spread(rows):
    return jnp.where(floor_div(iota((rows, 512), 1), HEADDIM) == iota((rows, 512), 0), 1.0, 0.0)


def conv_silu(window, taps):
    window = window.astype(jnp.float32)
    total = taps[3:4] * window[16:]
    for j in range(3):
        total = total + taps[j : j + 1] * pltpu.roll(window, 3 - j, 0)[16:]
    return jax.nn.silu(total)


def column_of(ref):
    return jnp.transpose(jnp.broadcast_to(ref[...], (8, 8)))[:, 0:1]


def mixer_local(m):
    spread = head_spread(8)
    low = iota((BLOCK, BLOCK), 0)
    high = iota((BLOCK, BLOCK), 1)
    causal = low >= high
    upper = jnp.where(low <= high, 1.0, 0.0)
    first = iota((BLOCK, 512), 1)
    first = first - 128 * floor_div(first, 128) < 64
    gain = exact_dot(jnp.broadcast_to(m.direct_gain[...], (8, 8)), spread)[0:1]
    rate = -jnp.exp(column_of(m.log_decay))
    step_bias = column_of(m.step_bias)
    value_taps = m.value_taps[...].astype(jnp.float32)
    map_taps = m.map_taps[...].astype(jnp.float32)
    m.state[...] = jnp.zeros_like(m.state)

    def block(b, prefix):
        start = pl.multiple_of(b * BLOCK, BLOCK)
        rows, window = pl.ds(start, BLOCK), pl.ds(start, BLOCK + 16)
        x = conv_silu(m.values[window, :], value_taps)
        in_maps = conv_silu(m.maps[0, window, :], map_taps[0])
        out_maps = conv_silu(m.maps[1, window, :], map_taps[1]).astype(jnp.bfloat16)
        m.out_maps[rows, :] = out_maps
        step_rows = softplus(m.step[:, rows] + step_bias)
        running_rows = exact_dot(rate * step_rows + m.increment[:, rows], upper)
        running = jnp.transpose(running_rows)
        step = jnp.transpose(step_rows)
        total = running[BLOCK - 1 : BLOCK, :]
        m.decay[rows, :] = jnp.exp(prefix + running)
        scaled = x * exact_dot(step, spread)
        to_end = (x * exact_dot(step * jnp.exp(total - running), spread)).astype(jnp.bfloat16)
        entered = exact_dot(jnp.exp(running), spread)
        left = jnp.where(first, scaled, 0.0).astype(jnp.bfloat16)
        right = jnp.where(first, 0.0, scaled).astype(jnp.bfloat16)
        for g in range(2):
            maps = slice(g * NSTATE, (g + 1) * NSTATE)
            wide = slice(g * 256, (g + 1) * 256)
            scores = lax.dot_general(
                out_maps[:, maps],
                in_maps[:, maps].astype(jnp.bfloat16),
                CONTRACT_LAST,
                preferred_element_type=jnp.float32,
            )
            carried = dot(out_maps[:, maps], m.state[:, wide].astype(jnp.bfloat16))
            for pair in range(2):
                mixes = []
                for h in (g * 4 + 2 * pair, g * 4 + 2 * pair + 1):
                    ahead = running[:, h : h + 1] - running_rows[h : h + 1, :]
                    between = jnp.exp(jnp.where(causal, ahead, -jnp.inf))
                    mixes.append((scores * between).astype(jnp.bfloat16))
                part = slice((g * 2 + pair) * 128, (g * 2 + pair + 1) * 128)
                inside = dot(
                    jnp.concatenate(mixes, axis=1),
                    jnp.concatenate([left[:, part], right[:, part]], axis=0),
                )
                m.mixed[rows, part] = (
                    inside
                    + carried[:, pair * 128 : (pair + 1) * 128] * entered[:, part]
                    + x[:, part] * gain[:, part]
                )
            turned = jnp.transpose(in_maps[:, maps]).astype(jnp.bfloat16)
            m.state[:, wide] = m.state[:, wide] * entered[BLOCK - 1 : BLOCK, wide] + dot(
                turned, to_end[:, wide]
            )
        return prefix + total

    prefix = lax.fori_loop(0, SEQ_BLOCKS, block, jnp.zeros((1, 8), jnp.float32))
    for j in range(8):
        m.state_out[j] = m.state[j * 16 : (j + 1) * 16, :].astype(jnp.bfloat16)
    heads = jnp.where(iota((8, 128), 0) == iota((8, 128), 1), 1.0, 0.0)
    m.decay_out[...] = exact_dot(jnp.broadcast_to(jnp.exp(prefix), (8, 8)), heads)


def plane_target(dxc):
    z, x, c = here()
    tx = lax.rem(x + lax.div(dxc, 2), 4)
    tc = lax.rem(c + lax.rem(dxc, 2), 2)
    return tx * 2 + tc, {"ep_1": tx, "ep_2": tc}


def plane_send(source, landing, send_sem, recv_sem, indexed):
    z, x, c = here()
    mine = x * 2 + c

    def send(dxc, unused):
        index, device = plane_target(dxc)
        pltpu.make_async_remote_copy(
            src_ref=source.at[index] if indexed else source,
            dst_ref=landing.at[mine],
            send_sem=send_sem,
            recv_sem=recv_sem,
            device_id=device,
            device_id_type=MESH_IDS,
        ).start()
        return unused

    lax.fori_loop(1, 8, send, 0)


def plane_wait(landing, send_sem, recv_sem):
    pltpu.make_async_remote_copy(
        src_ref=landing.at[pl.ds(0, 7)],
        dst_ref=landing.at[pl.ds(0, 7)],
        send_sem=send_sem,
        recv_sem=recv_sem,
        device_id=beside(1),
        device_id_type=MESH_IDS,
    ).wait()


def later_copy(m, d, which):
    source, landing = ((m.plane_state, m.early_state), (m.plane_decay, m.early_decay))[which]
    return pltpu.make_async_remote_copy(
        src_ref=source,
        dst_ref=landing.at[d - 1],
        send_sem=m.later_send.at[which, d - 1],
        recv_sem=m.later_recv.at[which, d - 1],
        device_id={"ep_0": lax.rem(lax.axis_index("ep_0") + d, 8)},
        device_id_type=MESH_IDS,
    )


def states_first(m):
    z, x, c = here()
    mine = x * 2 + c
    m.plane_states[mine] = m.state_out[mine]
    m.plane_decays[mine] = m.decay_out[...]
    plane_send(m.state_out, m.plane_states, m.plane_sems.at[0], m.plane_sems.at[1], True)
    plane_send(m.decay_out, m.plane_decays, m.plane_sems.at[2], m.plane_sems.at[3], False)


def states_second(m):
    plane_wait(m.plane_states, m.plane_sems.at[0], m.plane_sems.at[1])
    plane_wait(m.plane_decays, m.plane_sems.at[2], m.plane_sems.at[3])
    spread = head_spread(128)
    before = jnp.zeros((16, 512), jnp.float32)
    passed = jnp.ones((8, 128), jnp.float32)
    for j in range(8):
        m.before[j] = before
        m.passed[j] = passed
        decay = m.plane_decays[j]
        before = before * exact_dot(decay, spread)[0:1] + m.plane_states[j].astype(jnp.float32)
        passed = passed * decay
    m.plane_state[...] = before.astype(jnp.bfloat16)
    m.plane_decay[...] = passed
    z = lax.axis_index("ep_0")
    for d in range(1, 8):

        @pl.when(z + d < 8)
        def _():
            for which in range(2):
                later_copy(m, d, which).start()


def states_third(m):
    z, x, c = here()
    spread = head_spread(128)
    m.incoming[...] = jnp.zeros_like(m.incoming)
    for d in range(7, 0, -1):

        @pl.when(z >= d)
        def _():
            for which in range(2):
                later_copy(m, d, which).wait_recv()
            m.incoming[...] = m.incoming[...] * exact_dot(m.early_decay[d - 1], spread)[
                0:1
            ] + m.early_state[d - 1].astype(jnp.float32)

    incoming = m.incoming[...]
    for j in range(8):
        entering = m.before[j] + exact_dot(m.passed[j], spread)[0:1] * incoming
        m.answer_states[j] = entering.astype(jnp.bfloat16)
    mine = x * 2 + c
    m.entering[mine] = m.answer_states[mine]
    plane_send(m.answer_states, m.entering, m.plane_sems.at[4], m.plane_sems.at[5], True)
    for d in range(1, 8):

        @pl.when(z + d < 8)
        def _():
            for which in range(2):
                later_copy(m, d, which).wait_send()


def mixer_finish(m):
    plane_wait(m.entering, m.plane_sems.at[4], m.plane_sems.at[5])
    spread = head_spread(8)
    entering = m.entering[...].reshape(128, 512)

    def block(b, unused):
        rows = pl.ds(pl.multiple_of(b * BLOCK, BLOCK), BLOCK)
        decay = exact_dot(m.decay[rows, :], spread)
        for g in range(2):
            wide = slice(g * 256, (g + 1) * 256)
            carried = dot(m.out_maps[rows, g * NSTATE : (g + 1) * NSTATE], entering[:, wide])
            gated = (m.mixed[rows, wide] + carried * decay[:, wide]) * jax.nn.silu(
                m.gate[rows, wide].astype(jnp.float32)
            )
            scale = lax.rsqrt(jnp.mean(gated * gated, axis=1, keepdims=True) + EPSILON)
            m.result[rows, wide] = (gated * scale * m.norm_gain[:, wide]).astype(jnp.bfloat16)
        return unused

    lax.fori_loop(0, SEQ_BLOCKS, block, 0)


BF16 = jnp.bfloat16
F32 = jnp.float32

INPUTS = (
    "tokens_hbm",
    "expert_gain",
    "routes",
    "visit_weight",
    "gate_hbm",
    "up_hbm",
    "down_hbm",
    "values_hbm",
    "maps_hbm",
    "gate_pre_hbm",
    "step_hbm",
    "increment_hbm",
    "step_bias",
    "log_decay",
    "direct_gain",
    "value_taps",
    "map_taps",
    "norm_gain",
)
OUTPUTS = ("result", "routed_out")
SCRATCH = dict(
    tokens=pltpu.VMEM((256, 2048), BF16),
    normed=pltpu.VMEM((256, 2048), BF16),
    choice=pltpu.VMEM((768, 256), BF16),
    mix_high=pltpu.VMEM((256, 768), BF16),
    mix_low=pltpu.VMEM((256, 768), BF16),
    rows=pltpu.VMEM((768, 2048), BF16),
    sent=pltpu.VMEM((64, 48, 512), BF16),
    landed=pltpu.VMEM((64, 48, 512), BF16),
    hidden=pltpu.VMEM((4, 768, 256), BF16),
    answers=pltpu.VMEM((2, 64, 48, 256), BF16),
    returned=pltpu.VMEM((2, 64, 48, 256), BF16),
    total=pltpu.VMEM((256, 1024), F32),
    gate_slots=pltpu.VMEM((4, 2048, 256), BF16),
    up_slots=pltpu.VMEM((4, 2048, 256), BF16),
    down_slots=pltpu.VMEM((4, 2048, 256), BF16),
    values=pltpu.VMEM((1040, 512), BF16),
    maps=pltpu.VMEM((2, 1040, 256), BF16),
    gate=pltpu.VMEM((1024, 512), BF16),
    step=pltpu.VMEM((8, 1024), F32),
    increment=pltpu.VMEM((8, 1024), F32),
    decay=pltpu.VMEM((1024, 8), F32),
    mixed=pltpu.VMEM((1024, 512), F32),
    out_maps=pltpu.VMEM((1024, 256), BF16),
    state=pltpu.VMEM((128, 512), F32),
    state_out=pltpu.VMEM((8, 16, 512), BF16),
    decay_out=pltpu.VMEM((8, 128), F32),
    plane_states=pltpu.VMEM((8, 16, 512), BF16),
    plane_decays=pltpu.VMEM((8, 8, 128), F32),
    before=pltpu.VMEM((8, 16, 512), F32),
    passed=pltpu.VMEM((8, 8, 128), F32),
    plane_state=pltpu.VMEM((16, 512), BF16),
    plane_decay=pltpu.VMEM((8, 128), F32),
    early_state=pltpu.VMEM((7, 16, 512), BF16),
    early_decay=pltpu.VMEM((7, 8, 128), F32),
    incoming=pltpu.VMEM((16, 512), F32),
    answer_states=pltpu.VMEM((8, 16, 512), BF16),
    entering=pltpu.VMEM((8, 16, 512), BF16),
    local_sems=pltpu.SemaphoreType.DMA((9,)),
    near_send=pltpu.SemaphoreType.DMA((24,)),
    near_recv=pltpu.SemaphoreType.DMA((24,)),
    dispatch_sems=pltpu.SemaphoreType.DMA((4,)),
    answer_send=pltpu.SemaphoreType.DMA((4,)),
    answer_recv=pltpu.SemaphoreType.DMA((4,)),
    tail_send=pltpu.SemaphoreType.DMA((2,)),
    tail_recv=pltpu.SemaphoreType.DMA((2,)),
    plane_sems=pltpu.SemaphoreType.DMA((6,)),
    later_send=pltpu.SemaphoreType.DMA((2, 7)),
    later_recv=pltpu.SemaphoreType.DMA((2, 7)),
)


def kernel(*refs):
    m = types.SimpleNamespace(**dict(zip(INPUTS + OUTPUTS + tuple(SCRATCH), refs)))
    place = here()
    z, x, c = place
    me = z * 8 + x * 2 + c
    body = pl.ds(16, 1024)
    own_copies = [
        pltpu.make_async_copy(source, target, m.local_sems.at[i])
        for i, (source, target) in enumerate(
            (
                (m.tokens_hbm, m.tokens),
                (m.values_hbm, m.values.at[body]),
                (m.maps_hbm, m.maps.at[:, body]),
                (m.step_hbm, m.step),
                (m.increment_hbm, m.increment),
                (m.gate_pre_hbm, m.gate),
                (m.gate_hbm.at[0], m.gate_slots.at[0]),
                (m.up_hbm.at[0], m.up_slots.at[0]),
                (m.down_hbm.at[0], m.down_slots.at[0]),
            )
        )
    ]
    for copy in own_copies:
        copy.start()
    barrier = pltpu.get_barrier_semaphore()

    def greet(unused, device):
        pl.semaphore_signal(barrier, inc=1, device_id=device, device_id_type=MESH_IDS)

    for step in (1, 3):
        greet(0, beside(step))
    for_all_peers(greet)
    own_copies[0].wait()

    def norm_rows(i, unused):
        rows = pl.ds(pl.multiple_of(i * 32, 32), 32)
        values = m.tokens[rows, :].astype(jnp.float32)
        centered = values - jnp.mean(values, axis=1, keepdims=True)
        scale = lax.rsqrt(jnp.mean(centered * centered, axis=1, keepdims=True) + EPSILON)
        m.normed[rows, :] = (centered * scale * m.expert_gain[...]).astype(jnp.bfloat16)
        return unused

    lax.fori_loop(0, 8, norm_rows, 0)
    pl.semaphore_wait(barrier, 65)

    gate_near = Neighbours(m.gate_hbm, m.gate_slots, m.near_send, m.near_recv, 0, 0, 2048)
    up_near = Neighbours(m.up_hbm, m.up_slots, m.near_send, m.near_recv, 4, 0, 2048)
    down_near = [
        Neighbours(m.down_hbm, m.down_slots, m.near_send, m.near_recv, 8 + 4 * p, p * 512, 512)
        for p in range(4)
    ]
    gate_near.start()
    up_near.start()
    after = lax.rem(me + 1, 64)
    tails = [
        pltpu.make_async_remote_copy(
            src_ref=source,
            dst_ref=target,
            send_sem=m.tail_send.at[i],
            recv_sem=m.tail_recv.at[i],
            device_id={
                "ep_0": lax.div(after, 8),
                "ep_1": lax.rem(lax.div(after, 2), 4),
                "ep_2": lax.rem(after, 2),
            },
            device_id_type=MESH_IDS,
        )
        for i, (source, target) in enumerate(
            (
                (m.values_hbm.at[pl.ds(1008, 16)], m.values.at[pl.ds(0, 16)]),
                (m.maps_hbm.at[:, pl.ds(1008, 16)], m.maps.at[:, pl.ds(0, 16)]),
            )
        )
    ]
    for copy in tails:
        copy.start()

    experts = lax.broadcasted_iota(jnp.int32, (64, 256), 0)
    hits = [jnp.where(m.routes[k : k + 1, :] == experts, 1.0, 0.0) for k in range(2)]
    named = hits[0] + hits[1]
    earlier = jnp.where(iota((256, 256), 0) < iota((256, 256), 1), 1.0, 0.0).astype(jnp.bfloat16)
    slot = dot(named.astype(jnp.bfloat16), earlier)
    key = jnp.where(named > 0.5, slot, -1.0)
    peer = iota((64, 64), 0)
    plane = floor_div(peer, 8)
    turn = peer - 8.0 * plane
    ahead = jnp.zeros((64, 64), jnp.float32)
    for i, dz in enumerate(ORDER):
        ahead = ahead + jnp.where(turn == float(i), float(dz), 0.0)
    plane_x = floor_div(plane, 2)
    to_z = ahead + z.astype(jnp.float32)
    to_x = plane_x + x.astype(jnp.float32)
    to_c = plane - 2.0 * plane_x + c.astype(jnp.float32)
    to_z = to_z - 8.0 * floor_div(to_z, 8)
    to_x = to_x - 4.0 * floor_div(to_x, 4)
    to_c = to_c - 2.0 * floor_div(to_c, 2)
    expert_of = jnp.where(to_z * 8.0 + to_x * 2.0 + to_c == iota((64, 64), 1), 1.0, 0.0)
    expert_of = expert_of.astype(jnp.bfloat16)
    key = dot(expert_of, key.astype(jnp.bfloat16))
    spread = jnp.where(
        floor_div(iota((768, 64), 0), SLOTS) == iota((768, 64), 1), 1.0, 0.0
    ).astype(jnp.bfloat16)
    wanted = iota((768, 256), 0)
    wanted = wanted - SLOTS * floor_div(wanted, SLOTS)
    m.choice[...] = jnp.where(
        dot(spread, key.astype(jnp.bfloat16)) == wanted, 1.0, 0.0
    ).astype(jnp.bfloat16)
    matrix = repack_matrix()

    def pick(p, unused):
        columns = pl.ds(pl.multiple_of(p * 512, 512), 512)
        m.rows[:, columns] = dot(m.choice[...], m.normed[:, columns]).astype(jnp.bfloat16)
        return unused

    lax.fori_loop(0, 4, pick, 0)

    def pack_dispatch(dxc):
        for g in range(2):
            rows = m.rows[pl.ds(pl.multiple_of(dxc * 96 + g * 48, 16), 48), :]
            m.sent[pl.ds(dxc * 8 + g * 4, 4)] = pack_group(rows, matrix, 512)

    def send_dispatch(dxc, half):
        send_group(m.sent, m.landed, dxc, m.dispatch_sems.at[half], m.dispatch_sems.at[2 + half], 1)

    pack_dispatch(0)
    pack_dispatch(1)
    send_dispatch(0, 0)

    def dispatch_first(dxc, unused):
        pack_dispatch(dxc + 1)
        send_dispatch(dxc, 0)
        return unused

    def dispatch_second(dxc, unused):
        pack_dispatch(dxc + 1)
        send_dispatch(dxc, 1)
        return unused

    lax.fori_loop(1, 4, dispatch_first, 0)
    lax.fori_loop(4, 7, dispatch_second, 0)
    m.landed[7] = m.sent[7]
    send_dispatch(jnp.int32(7), 1)

    for copy in own_copies[1:5]:
        copy.wait()
    for copy in tails:
        copy.wait_recv()
    m.values[0:16, :] = jnp.where(me > 0, m.values[0:16, :], jnp.zeros((16, 512), jnp.bfloat16))
    m.maps[:, 0:16, :] = jnp.where(me > 0, m.maps[:, 0:16, :], jnp.zeros((2, 16, 256), jnp.bfloat16))
    mixer_local(m)
    states_first(m)

    weights = m.visit_weight[0:1, :] * hits[0] + m.visit_weight[1:2, :] * hits[1]
    spread_columns = jnp.where(
        floor_div(iota((64, 768), 1), SLOTS) == iota((64, 768), 0), 1.0, 0.0
    ).astype(jnp.bfloat16)
    wanted = iota((256, 768), 1)
    wanted = wanted - SLOTS * floor_div(wanted, SLOTS)
    mine = dot(jnp.transpose(key).astype(jnp.bfloat16), spread_columns) == wanted
    high = weights.astype(jnp.bfloat16)
    low = (weights - high.astype(jnp.float32)).astype(jnp.bfloat16)
    for part, target in ((high, m.mix_high), (low, m.mix_low)):
        turned = jnp.transpose(dot(expert_of, part)).astype(jnp.bfloat16)
        target[...] = jnp.where(mine, dot(turned, spread_columns), 0.0).astype(jnp.bfloat16)

    for copy in own_copies[5:]:
        copy.wait()
    gate_near.forward()
    up_near.forward()
    down_near[0].start()
    down_near[1].start()
    states_second(m)
    gate_near.arrive()
    up_near.arrive()

    def activate(half):
        half_bytes(m.sent, m.landed, half, m.dispatch_sems.at[half], m.dispatch_sems.at[2 + half]).wait()
        unpack_half(m.landed, m.rows, matrix, half, 0, 512)

        def one(j, unused):
            rows = m.rows[half * 384 : (half + 1) * 384, :]
            opened = dot(rows, m.gate_slots[j])
            raised = dot(rows, m.up_slots[j])
            m.hidden[j, half * 384 : (half + 1) * 384, :] = (jax.nn.silu(opened) * raised).astype(
                jnp.bfloat16
            )
            return unused

        lax.fori_loop(0, 4, one, 0)

    def answer(half, p):
        inside = slice(half * 384, (half + 1) * 384)

        def one(n, unused):
            lines = pl.ds(pl.multiple_of(p * 1024 + n * 256, 256), 256)
            total = jnp.zeros((384, 256), jnp.float32)
            for j in range(4):
                total = total + lax.dot_general(
                    m.hidden[j, inside],
                    m.down_slots[j, lines, :],
                    CONTRACT_LAST,
                    preferred_element_type=jnp.float32,
                )
            m.rows[inside, lines] = total.astype(jnp.bfloat16)
            return unused

        lax.fori_loop(0, 4, one, 0)
        for g in range(half * 8, half * 8 + 8):
            m.answers[p, g * 4 : g * 4 + 4] = pack_group(
                m.rows[g * 48 : (g + 1) * 48, p * 1024 : (p + 1) * 1024], matrix, 256
            )
        which = 2 * p + half
        sems = (m.answer_send.at[which], m.answer_recv.at[which])
        if half == 0:
            m.returned[p, 7] = m.answers[p, 7]
            send_group(m.answers.at[p], m.returned.at[p], 0, *sems, -1)

        def some(dxc, unused):
            send_group(m.answers.at[p], m.returned.at[p], dxc, *sems, -1)
            return unused

        lax.fori_loop(max(1, half * 4), half * 4 + 4, some, 0)

    activate(0)
    down_near[0].forward()
    down_near[1].forward()
    down_near[2].start()
    down_near[3].start()
    activate(1)
    states_third(m)
    down_near[0].arrive()
    down_near[1].arrive()
    answer(0, 0)
    answer(1, 0)
    down_near[2].forward()
    down_near[3].forward()
    down_near[2].arrive()
    down_near[3].arrive()
    answer(0, 1)
    answer(1, 1)
    mixer_finish(m)

    for p in range(2):
        lines = pl.ds(p * 1024, 1024)
        for half in range(2):
            which = 2 * p + half
            half_bytes(
                m.answers.at[p],
                m.returned.at[p],
                half,
                m.answer_send.at[which],
                m.answer_recv.at[which],
            ).wait()
            unpack_half(m.returned.at[p], m.rows, matrix, half, p * 1024, 256)
            inside = slice(half * 384, (half + 1) * 384)
            share = dot(m.mix_high[:, inside], m.rows[inside, lines]) + dot(
                m.mix_low[:, inside], m.rows[inside, lines]
            )
            if half == 0:
                m.total[...] = share
            else:
                m.routed_out[:, lines] = (m.total[...] + share).astype(jnp.bfloat16)

    for near in [gate_near, up_near] + down_near:
        near.drain()
    for copy in tails:
        copy.wait_send()


def body(
    first_micro_values,
    group_state_maps,
    gate_preactivation,
    step_preactivation,
    head_step_bias,
    head_log_decay,
    decay_increment,
    head_direct_gain,
    convolution_value_taps,
    convolution_map_taps,
    grouped_norm_gain,
    second_micro_tokens,
    expert_norm_gain,
    routes,
    visit_weight,
    gate_weight_table,
    up_weight_table,
    down_weight_table,
):
    operands = (
        second_micro_tokens,
        expert_norm_gain.reshape(1, -1),
        routes.T,
        visit_weight.T,
        gate_weight_table,
        up_weight_table,
        down_weight_table,
        first_micro_values,
        group_state_maps,
        gate_preactivation,
        step_preactivation.T,
        decay_increment.T,
        head_step_bias.reshape(1, -1),
        head_log_decay.reshape(1, -1),
        head_direct_gain.reshape(1, -1),
        convolution_value_taps,
        convolution_map_taps,
        grouped_norm_gain.reshape(1, -1),
    )
    vmem = pl.BlockSpec(memory_space=pltpu.VMEM)
    hbm = pl.BlockSpec(memory_space=pl.ANY)
    return pl.pallas_call(
        kernel,
        out_shape=(
            jax.ShapeDtypeStruct((1024, 512), BF16),
            jax.ShapeDtypeStruct((256, 2048), BF16),
        ),
        in_specs=[hbm if name.endswith("_hbm") else vmem for name in INPUTS],
        out_specs=(vmem, vmem),
        scratch_shapes=list(SCRATCH.values()),
        compiler_params=pltpu.CompilerParams(
            collective_id=0, has_side_effects=True, vmem_limit_bytes=60 * 2**20
        ),
    )(*operands)


def solution(mesh):
    torus = Mesh(mesh.devices.reshape(8, 4, 2, mesh.shape["tp"]), ("ep_0", "ep_1", "ep_2", "tp"))
    in_specs = (
        P(EP, "tp"),
        P(None, EP, "tp"),
        P(EP, "tp"),
        P(EP, "tp"),
        P("tp"),
        P("tp"),
        P(EP, "tp"),
        P("tp"),
        P(None, "tp"),
        P(None, None, "tp"),
        P("tp"),
        P(EP_TP, None),
        P(),
        P(EP_TP, None),
        P(EP_TP, None),
        P(EP, None, "tp"),
        P(EP, None, "tp"),
        P(EP, None, "tp"),
    )
    out_specs = (P(EP, "tp"), P(EP_TP, None))
    return jax.shard_map(body, mesh=torus, in_specs=in_specs, out_specs=out_specs, check_vma=False)
```

```python
import types

import jax
import jax.numpy as jnp
from jax import lax
from jax.experimental import pallas as pl
from jax.experimental.pallas import tpu as pltpu
from jax.sharding import Mesh
from jax.sharding import PartitionSpec as P

HEADDIM = 64
NSTATE = 128
BLOCK = 128
SEQ_BLOCKS = 8
EP = ("ep_0", "ep_1", "ep_2")
EP_TP = ("ep_0", "ep_1", "ep_2", "tp")


EPSILON = 1e-05
CONTRACT_LAST = (((1,), (1,)), ((), ()))


SLOTS = 12
CHUNKS = ((0, 512), (512, 512), (1024, 512), (1536, 512))
ORDER = (4, 1, 7, 3, 5, 2, 6, 0)
MESH_IDS = pl.DeviceIdType.MESH


def here():
    return (lax.axis_index("ep_0"), lax.axis_index("ep_1"), lax.axis_index("ep_2"))


def beside(step):
    return {"tp": lax.rem(lax.axis_index("tp") + step, 4)}


def around(place, dz, dxc, sign):
    z, x, c = place
    return {
        "ep_0": lax.rem(z + (dz if sign > 0 else 8 - dz), 8),
        "ep_1": lax.rem(x + (lax.div(dxc, 2) if sign > 0 else 4 - lax.div(dxc, 2)), 4),
        "ep_2": lax.rem(c + lax.rem(dxc, 2), 2),
    }


def for_peers(dxc, act, sign):
    place = here()
    for i, dz in enumerate(ORDER):
        act(i, around(place, dz, dxc, sign))


def for_all_peers(act):
    place = here()
    for i, dz in enumerate(ORDER[:7]):
        act(i, around(place, dz, 0, 1))

    def some(dxc, unused):
        for_peers(dxc, lambda i, device: act(dxc * 8 + i, device), 1)
        return unused

    lax.fori_loop(1, 8, some, 0)


def row_copy(source, landing, index, send_sem, recv_sem, device):
    return pltpu.make_async_remote_copy(
        src_ref=source.at[index],
        dst_ref=landing.at[index],
        send_sem=send_sem,
        recv_sem=recv_sem,
        device_id=device,
        device_id_type=MESH_IDS,
    )


def send_group(source, landing, dxc, send_sem, recv_sem, sign):
    place = here()
    first = isinstance(dxc, int) and dxc == 0
    for i, dz in enumerate(ORDER[:7] if first else ORDER):
        device = around(place, dz, dxc, sign)
        row_copy(source, landing, dxc * 8 + i, send_sem, recv_sem, device).start()


def half_bytes(source, landing, half, send_sem, recv_sem):
    rows = pl.ds(0, 31) if half == 0 else pl.ds(32, 32)
    return pltpu.make_async_remote_copy(
        src_ref=source.at[rows],
        dst_ref=landing.at[rows],
        send_sem=send_sem,
        recv_sem=recv_sem,
        device_id=beside(1),
        device_id_type=MESH_IDS,
    )


def floor_div(values, divisor):
    return jnp.floor((values + 0.5) * (1.0 / divisor))


def iota(shape, axis):
    return lax.broadcasted_iota(jnp.int32, shape, axis).astype(jnp.float32)


def dot(a, b):
    return jnp.dot(a, b, preferred_element_type=jnp.float32)


def repack_matrix():
    size = 16 * SLOTS
    row = iota((size, size), 0)
    outer = floor_div(row, 4 * SLOTS)
    rest = row - 4 * SLOTS * outer
    inner = floor_div(rest, SLOTS)
    partner = inner * (4 * SLOTS) + outer * SLOTS + (rest - inner * SLOTS)
    return jnp.where(iota((size, size), 1) == partner, 1.0, 0.0).astype(jnp.bfloat16)


def pack_group(rows, matrix, width):
    tall = jnp.concatenate([rows[:, p * width : (p + 1) * width] for p in range(4)], axis=0)
    return dot(matrix, tall).astype(jnp.bfloat16).reshape(4, 48, width)


def unpack_half(source, landing, matrix, half, column, width):
    for g in range(half * 8, half * 8 + 8):
        rows = dot(matrix, source[g * 4 : g * 4 + 4].reshape(192, width)).astype(jnp.bfloat16)
        for p in range(4):
            landing[g * 48 : (g + 1) * 48, column + p * width : column + (p + 1) * width] = rows[
                p * 48 : (p + 1) * 48
            ]


class Neighbours:
    def __init__(self, own, slots, send_sems, recv_sems, first, start, size):
        half = size // 2
        whole, low, high = pl.ds(start, size), pl.ds(start, half), pl.ds(start + half, half)

        def copy(which, source, landing, step):
            return pltpu.make_async_remote_copy(
                src_ref=source,
                dst_ref=landing,
                send_sem=send_sems.at[first + which],
                recv_sem=recv_sems.at[first + which],
                device_id=beside(step),
                device_id_type=MESH_IDS,
            )

        self.near = (
            copy(0, own.at[0, whole], slots.at[1, whole], 1),
            copy(1, own.at[0, whole], slots.at[2, whole], 3),
        )
        self.far = (
            copy(2, slots.at[1, low], slots.at[3, low], 1),
            copy(3, slots.at[2, high], slots.at[3, high], 3),
        )

    def start(self):
        for copy in self.near:
            copy.start()

    def forward(self):
        for arrived, onward in zip(self.near, self.far):
            arrived.wait_recv()
            onward.start()

    def arrive(self):
        for copy in self.far:
            copy.wait_recv()

    def drain(self):
        for copy in self.near + self.far:
            copy.wait_send()


def exact_dot(a, b):
    return jnp.dot(a, b, precision=lax.Precision.HIGHEST, preferred_element_type=jnp.float32)


def softplus(values):
    small = jnp.exp(-jnp.abs(values))
    ratio = small / (2.0 + small)
    square = ratio * ratio
    series = 1.0 / 13.0
    for odd in (11.0, 9.0, 7.0, 5.0, 3.0, 1.0):
        series = series * square + 1.0 / odd
    return jnp.maximum(values, 0.0) + 2.0 * ratio * series


def head_spread(rows):
    return jnp.where(floor_div(iota((rows, 512), 1), HEADDIM) == iota((rows, 512), 0), 1.0, 0.0)


def conv_silu(window, taps):
    window = window.astype(jnp.float32)
    total = taps[3:4] * window[16:]
    for j in range(3):
        total = total + taps[j : j + 1] * pltpu.roll(window, 3 - j, 0)[16:]
    return jax.nn.silu(total)


def column_of(ref):
    return jnp.transpose(jnp.broadcast_to(ref[...], (8, 8)))[:, 0:1]


def mixer_local(m):
    spread = head_spread(8)
    low = iota((BLOCK, BLOCK), 0)
    high = iota((BLOCK, BLOCK), 1)
    causal = low >= high
    upper = jnp.where(low <= high, 1.0, 0.0)
    first = iota((BLOCK, 512), 1)
    first = first - 128 * floor_div(first, 128) < 64
    gain = exact_dot(jnp.broadcast_to(m.direct_gain[...], (8, 8)), spread)[0:1]
    rate = -jnp.exp(column_of(m.log_decay))
    step_bias = column_of(m.step_bias)
    value_taps = m.value_taps[...].astype(jnp.float32)
    map_taps = m.map_taps[...].astype(jnp.float32)
    m.state[...] = jnp.zeros_like(m.state)

    def block(b, prefix):
        start = pl.multiple_of(b * BLOCK, BLOCK)
        rows, window = pl.ds(start, BLOCK), pl.ds(start, BLOCK + 16)
        x = conv_silu(m.values[window, :], value_taps)
        in_maps = conv_silu(m.maps[0, window, :], map_taps[0])
        out_maps = conv_silu(m.maps[1, window, :], map_taps[1]).astype(jnp.bfloat16)
        m.out_maps[rows, :] = out_maps
        step_rows = softplus(m.step[:, rows] + step_bias)
        running_rows = exact_dot(rate * step_rows + m.increment[:, rows], upper)
        running = jnp.transpose(running_rows)
        step = jnp.transpose(step_rows)
        total = running[BLOCK - 1 : BLOCK, :]
        m.decay[rows, :] = jnp.exp(prefix + running)
        scaled = x * exact_dot(step, spread)
        to_end = (x * exact_dot(step * jnp.exp(total - running), spread)).astype(jnp.bfloat16)
        entered = exact_dot(jnp.exp(running), spread)
        left = jnp.where(first, scaled, 0.0).astype(jnp.bfloat16)
        right = jnp.where(first, 0.0, scaled).astype(jnp.bfloat16)
        for g in range(2):
            maps = slice(g * NSTATE, (g + 1) * NSTATE)
            wide = slice(g * 256, (g + 1) * 256)
            scores = lax.dot_general(
                out_maps[:, maps],
                in_maps[:, maps].astype(jnp.bfloat16),
                CONTRACT_LAST,
                preferred_element_type=jnp.float32,
            )
            carried = dot(out_maps[:, maps], m.state[:, wide].astype(jnp.bfloat16))
            for pair in range(2):
                mixes = []
                for h in (g * 4 + 2 * pair, g * 4 + 2 * pair + 1):
                    ahead = running[:, h : h + 1] - running_rows[h : h + 1, :]
                    between = jnp.exp(jnp.where(causal, ahead, -jnp.inf))
                    mixes.append((scores * between).astype(jnp.bfloat16))
                part = slice((g * 2 + pair) * 128, (g * 2 + pair + 1) * 128)
                inside = dot(
                    jnp.concatenate(mixes, axis=1),
                    jnp.concatenate([left[:, part], right[:, part]], axis=0),
                )
                m.mixed[rows, part] = (
                    inside
                    + carried[:, pair * 128 : (pair + 1) * 128] * entered[:, part]
                    + x[:, part] * gain[:, part]
                )
            turned = jnp.transpose(in_maps[:, maps]).astype(jnp.bfloat16)
            m.state[:, wide] = m.state[:, wide] * entered[BLOCK - 1 : BLOCK, wide] + dot(
                turned, to_end[:, wide]
            )
        return prefix + total

    prefix = lax.fori_loop(0, SEQ_BLOCKS, block, jnp.zeros((1, 8), jnp.float32))
    for j in range(8):
        m.state_out[j] = m.state[j * 16 : (j + 1) * 16, :].astype(jnp.bfloat16)
    heads = jnp.where(iota((8, 128), 0) == iota((8, 128), 1), 1.0, 0.0)
    m.decay_out[...] = exact_dot(jnp.broadcast_to(jnp.exp(prefix), (8, 8)), heads)


def plane_target(dxc):
    z, x, c = here()
    tx = lax.rem(x + lax.div(dxc, 2), 4)
    tc = lax.rem(c + lax.rem(dxc, 2), 2)
    return tx * 2 + tc, {"ep_1": tx, "ep_2": tc}


def plane_send(source, landing, send_sem, recv_sem, indexed):
    z, x, c = here()
    mine = x * 2 + c

    def send(dxc, unused):
        index, device = plane_target(dxc)
        pltpu.make_async_remote_copy(
            src_ref=source.at[index] if indexed else source,
            dst_ref=landing.at[mine],
            send_sem=send_sem,
            recv_sem=recv_sem,
            device_id=device,
            device_id_type=MESH_IDS,
        ).start()
        return unused

    lax.fori_loop(1, 8, send, 0)


def plane_wait(landing, send_sem, recv_sem):
    pltpu.make_async_remote_copy(
        src_ref=landing.at[pl.ds(0, 7)],
        dst_ref=landing.at[pl.ds(0, 7)],
        send_sem=send_sem,
        recv_sem=recv_sem,
        device_id=beside(1),
        device_id_type=MESH_IDS,
    ).wait()


def later_copy(m, d, which):
    source, landing = ((m.plane_state, m.early_state), (m.plane_decay, m.early_decay))[which]
    return pltpu.make_async_remote_copy(
        src_ref=source,
        dst_ref=landing.at[d - 1],
        send_sem=m.later_send.at[which, d - 1],
        recv_sem=m.later_recv.at[which, d - 1],
        device_id={"ep_0": lax.rem(lax.axis_index("ep_0") + d, 8)},
        device_id_type=MESH_IDS,
    )


def states_first(m):
    z, x, c = here()
    mine = x * 2 + c
    m.plane_states[mine] = m.state_out[mine]
    m.plane_decays[mine] = m.decay_out[...]
    plane_send(m.state_out, m.plane_states, m.plane_sems.at[0], m.plane_sems.at[1], True)
    plane_send(m.decay_out, m.plane_decays, m.plane_sems.at[2], m.plane_sems.at[3], False)


def states_second(m):
    plane_wait(m.plane_states, m.plane_sems.at[0], m.plane_sems.at[1])
    plane_wait(m.plane_decays, m.plane_sems.at[2], m.plane_sems.at[3])
    spread = head_spread(128)
    before = jnp.zeros((16, 512), jnp.float32)
    passed = jnp.ones((8, 128), jnp.float32)
    for j in range(8):
        m.before[j] = before
        m.passed[j] = passed
        decay = m.plane_decays[j]
        before = before * exact_dot(decay, spread)[0:1] + m.plane_states[j].astype(jnp.float32)
        passed = passed * decay
    m.plane_state[...] = before.astype(jnp.bfloat16)
    m.plane_decay[...] = passed
    z = lax.axis_index("ep_0")
    for d in range(1, 8):

        @pl.when(z + d < 8)
        def _():
            for which in range(2):
                later_copy(m, d, which).start()


def states_third(m):
    z, x, c = here()
    spread = head_spread(128)
    m.incoming[...] = jnp.zeros_like(m.incoming)
    for d in range(7, 0, -1):

        @pl.when(z >= d)
        def _():
            for which in range(2):
                later_copy(m, d, which).wait_recv()
            m.incoming[...] = m.incoming[...] * exact_dot(m.early_decay[d - 1], spread)[
                0:1
            ] + m.early_state[d - 1].astype(jnp.float32)

    incoming = m.incoming[...]
    for j in range(8):
        entering = m.before[j] + exact_dot(m.passed[j], spread)[0:1] * incoming
        m.answer_states[j] = entering.astype(jnp.bfloat16)
    mine = x * 2 + c
    m.entering[mine] = m.answer_states[mine]
    plane_send(m.answer_states, m.entering, m.plane_sems.at[4], m.plane_sems.at[5], True)
    for d in range(1, 8):

        @pl.when(z + d < 8)
        def _():
            for which in range(2):
                later_copy(m, d, which).wait_send()


def mixer_finish(m):
    plane_wait(m.entering, m.plane_sems.at[4], m.plane_sems.at[5])
    spread = head_spread(8)
    entering = m.entering[...].reshape(128, 512)

    def block(b, unused):
        rows = pl.ds(pl.multiple_of(b * BLOCK, BLOCK), BLOCK)
        decay = exact_dot(m.decay[rows, :], spread)
        for g in range(2):
            wide = slice(g * 256, (g + 1) * 256)
            carried = dot(m.out_maps[rows, g * NSTATE : (g + 1) * NSTATE], entering[:, wide])
            gated = (m.mixed[rows, wide] + carried * decay[:, wide]) * jax.nn.silu(
                m.gate[rows, wide].astype(jnp.float32)
            )
            scale = lax.rsqrt(jnp.mean(gated * gated, axis=1, keepdims=True) + EPSILON)
            m.result[rows, wide] = (gated * scale * m.norm_gain[:, wide]).astype(jnp.bfloat16)
        return unused

    lax.fori_loop(0, SEQ_BLOCKS, block, 0)


BF16 = jnp.bfloat16
F32 = jnp.float32

INPUTS = (
    "tokens_hbm",
    "expert_gain",
    "routes",
    "visit_weight",
    "gate_hbm",
    "up_hbm",
    "down_hbm",
    "values_hbm",
    "maps_hbm",
    "gate_pre_hbm",
    "step_hbm",
    "increment_hbm",
    "step_bias",
    "log_decay",
    "direct_gain",
    "value_taps",
    "map_taps",
    "norm_gain",
)
OUTPUTS = ("result", "routed_out")
SCRATCH = dict(
    tokens=pltpu.VMEM((256, 2048), BF16),
    normed=pltpu.VMEM((256, 2048), BF16),
    choice=pltpu.VMEM((768, 256), BF16),
    mix_high=pltpu.VMEM((256, 768), BF16),
    mix_low=pltpu.VMEM((256, 768), BF16),
    rows=pltpu.VMEM((768, 2048), BF16),
    sent=pltpu.VMEM((64, 48, 512), BF16),
    landed=pltpu.VMEM((64, 48, 512), BF16),
    hidden=pltpu.VMEM((4, 768, 256), BF16),
    answers_0=pltpu.VMEM((64, 48, 128), BF16),
    answers_1=pltpu.VMEM((64, 48, 128), BF16),
    answers_2=pltpu.VMEM((64, 48, 128), BF16),
    answers_3=pltpu.VMEM((64, 48, 128), BF16),
    returned_0=pltpu.VMEM((64, 48, 128), BF16),
    returned_1=pltpu.VMEM((64, 48, 128), BF16),
    returned_2=pltpu.VMEM((64, 48, 128), BF16),
    returned_3=pltpu.VMEM((64, 48, 128), BF16),
    total=pltpu.VMEM((256, 512), F32),
    gate_slots=pltpu.VMEM((4, 2048, 256), BF16),
    up_slots=pltpu.VMEM((4, 2048, 256), BF16),
    down_slots=pltpu.VMEM((4, 2048, 256), BF16),
    values=pltpu.VMEM((1040, 512), BF16),
    maps=pltpu.VMEM((2, 1040, 256), BF16),
    gate=pltpu.VMEM((1024, 512), BF16),
    step=pltpu.VMEM((8, 1024), F32),
    increment=pltpu.VMEM((8, 1024), F32),
    decay=pltpu.VMEM((1024, 8), F32),
    mixed=pltpu.VMEM((1024, 512), F32),
    out_maps=pltpu.VMEM((1024, 256), BF16),
    state=pltpu.VMEM((128, 512), F32),
    state_out=pltpu.VMEM((8, 16, 512), BF16),
    decay_out=pltpu.VMEM((8, 128), F32),
    plane_states=pltpu.VMEM((8, 16, 512), BF16),
    plane_decays=pltpu.VMEM((8, 8, 128), F32),
    before=pltpu.VMEM((8, 16, 512), F32),
    passed=pltpu.VMEM((8, 8, 128), F32),
    plane_state=pltpu.VMEM((16, 512), BF16),
    plane_decay=pltpu.VMEM((8, 128), F32),
    early_state=pltpu.VMEM((7, 16, 512), BF16),
    early_decay=pltpu.VMEM((7, 8, 128), F32),
    incoming=pltpu.VMEM((16, 512), F32),
    answer_states=pltpu.VMEM((8, 16, 512), BF16),
    entering=pltpu.VMEM((8, 16, 512), BF16),
    local_sems=pltpu.SemaphoreType.DMA((9,)),
    near_send=pltpu.SemaphoreType.DMA((24,)),
    near_recv=pltpu.SemaphoreType.DMA((24,)),
    dispatch_sems=pltpu.SemaphoreType.DMA((4,)),
    answer_send=pltpu.SemaphoreType.DMA((8,)),
    answer_recv=pltpu.SemaphoreType.DMA((8,)),
    tail_send=pltpu.SemaphoreType.DMA((2,)),
    tail_recv=pltpu.SemaphoreType.DMA((2,)),
    plane_sems=pltpu.SemaphoreType.DMA((6,)),
    later_send=pltpu.SemaphoreType.DMA((2, 7)),
    later_recv=pltpu.SemaphoreType.DMA((2, 7)),
)


def kernel(*refs):
    m = types.SimpleNamespace(**dict(zip(INPUTS + OUTPUTS + tuple(SCRATCH), refs)))
    place = here()
    z, x, c = place
    me = z * 8 + x * 2 + c
    body = pl.ds(16, 1024)
    own_copies = [
        pltpu.make_async_copy(source, target, m.local_sems.at[i])
        for i, (source, target) in enumerate(
            (
                (m.tokens_hbm, m.tokens),
                (m.values_hbm, m.values.at[body]),
                (m.maps_hbm, m.maps.at[:, body]),
                (m.step_hbm, m.step),
                (m.increment_hbm, m.increment),
                (m.gate_pre_hbm, m.gate),
                (m.gate_hbm.at[0], m.gate_slots.at[0]),
                (m.up_hbm.at[0], m.up_slots.at[0]),
                (m.down_hbm.at[0], m.down_slots.at[0]),
            )
        )
    ]
    for copy in own_copies:
        copy.start()
    barrier = pltpu.get_barrier_semaphore()

    def greet(unused, device):
        pl.semaphore_signal(barrier, inc=1, device_id=device, device_id_type=MESH_IDS)

    for step in (1, 3):
        greet(0, beside(step))
    for_all_peers(greet)
    pl.semaphore_wait(barrier, 65)

    gate_near = Neighbours(m.gate_hbm, m.gate_slots, m.near_send, m.near_recv, 0, 0, 2048)
    up_near = Neighbours(m.up_hbm, m.up_slots, m.near_send, m.near_recv, 4, 0, 2048)
    down_near = [
        Neighbours(m.down_hbm, m.down_slots, m.near_send, m.near_recv, 8 + 4 * p, p * 512, 512)
        for p in range(4)
    ]
    gate_near.start()
    up_near.start()
    down_near[0].start()
    after = lax.rem(me + 1, 64)
    tails = [
        pltpu.make_async_remote_copy(
            src_ref=source,
            dst_ref=target,
            send_sem=m.tail_send.at[i],
            recv_sem=m.tail_recv.at[i],
            device_id={
                "ep_0": lax.div(after, 8),
                "ep_1": lax.rem(lax.div(after, 2), 4),
                "ep_2": lax.rem(after, 2),
            },
            device_id_type=MESH_IDS,
        )
        for i, (source, target) in enumerate(
            (
                (m.values_hbm.at[pl.ds(1008, 16)], m.values.at[pl.ds(0, 16)]),
                (m.maps_hbm.at[:, pl.ds(1008, 16)], m.maps.at[:, pl.ds(0, 16)]),
            )
        )
    ]
    for copy in tails:
        copy.start()

    own_copies[0].wait()

    def norm_rows(i, unused):
        rows = pl.ds(pl.multiple_of(i * 32, 32), 32)
        values = m.tokens[rows, :].astype(jnp.float32)
        centered = values - jnp.mean(values, axis=1, keepdims=True)
        scale = lax.rsqrt(jnp.mean(centered * centered, axis=1, keepdims=True) + EPSILON)
        m.normed[rows, :] = (centered * scale * m.expert_gain[...]).astype(jnp.bfloat16)
        return unused

    lax.fori_loop(0, 8, norm_rows, 0)

    experts = lax.broadcasted_iota(jnp.int32, (64, 256), 0)
    hits = [jnp.where(m.routes[k : k + 1, :] == experts, 1.0, 0.0) for k in range(2)]
    named = hits[0] + hits[1]
    earlier = jnp.where(iota((256, 256), 0) < iota((256, 256), 1), 1.0, 0.0).astype(jnp.bfloat16)
    slot = dot(named.astype(jnp.bfloat16), earlier)
    key = jnp.where(named > 0.5, slot, -1.0)
    peer = iota((64, 64), 0)
    plane = floor_div(peer, 8)
    turn = peer - 8.0 * plane
    ahead = jnp.zeros((64, 64), jnp.float32)
    for i, dz in enumerate(ORDER):
        ahead = ahead + jnp.where(turn == float(i), float(dz), 0.0)
    plane_x = floor_div(plane, 2)
    to_z = ahead + z.astype(jnp.float32)
    to_x = plane_x + x.astype(jnp.float32)
    to_c = plane - 2.0 * plane_x + c.astype(jnp.float32)
    to_z = to_z - 8.0 * floor_div(to_z, 8)
    to_x = to_x - 4.0 * floor_div(to_x, 4)
    to_c = to_c - 2.0 * floor_div(to_c, 2)
    expert_of = jnp.where(to_z * 8.0 + to_x * 2.0 + to_c == iota((64, 64), 1), 1.0, 0.0)
    expert_of = expert_of.astype(jnp.bfloat16)
    key = dot(expert_of, key.astype(jnp.bfloat16))
    spread = jnp.where(
        floor_div(iota((768, 64), 0), SLOTS) == iota((768, 64), 1), 1.0, 0.0
    ).astype(jnp.bfloat16)
    wanted = iota((768, 256), 0)
    wanted = wanted - SLOTS * floor_div(wanted, SLOTS)
    m.choice[...] = jnp.where(
        dot(spread, key.astype(jnp.bfloat16)) == wanted, 1.0, 0.0
    ).astype(jnp.bfloat16)
    matrix = repack_matrix()

    def pick(p, unused):
        columns = pl.ds(pl.multiple_of(p * 512, 512), 512)
        m.rows[:, columns] = dot(m.choice[...], m.normed[:, columns]).astype(jnp.bfloat16)
        return unused

    lax.fori_loop(0, 4, pick, 0)

    def pack_dispatch(dxc):
        for g in range(2):
            rows = m.rows[pl.ds(pl.multiple_of(dxc * 96 + g * 48, 16), 48), :]
            m.sent[pl.ds(dxc * 8 + g * 4, 4)] = pack_group(rows, matrix, 512)

    def send_dispatch(dxc, half):
        send_group(m.sent, m.landed, dxc, m.dispatch_sems.at[half], m.dispatch_sems.at[2 + half], 1)

    pack_dispatch(0)
    pack_dispatch(1)
    send_dispatch(0, 0)

    def dispatch_first(dxc, unused):
        pack_dispatch(dxc + 1)
        send_dispatch(dxc, 0)
        return unused

    def dispatch_second(dxc, unused):
        pack_dispatch(dxc + 1)
        send_dispatch(dxc, 1)
        return unused

    lax.fori_loop(1, 4, dispatch_first, 0)
    lax.fori_loop(4, 7, dispatch_second, 0)
    m.landed[7] = m.sent[7]
    send_dispatch(jnp.int32(7), 1)

    for copy in own_copies[1:5]:
        copy.wait()
    for copy in tails:
        copy.wait_recv()
    m.values[0:16, :] = jnp.where(me > 0, m.values[0:16, :], jnp.zeros((16, 512), jnp.bfloat16))
    m.maps[:, 0:16, :] = jnp.where(me > 0, m.maps[:, 0:16, :], jnp.zeros((2, 16, 256), jnp.bfloat16))
    mixer_local(m)
    states_first(m)

    weights = m.visit_weight[0:1, :] * hits[0] + m.visit_weight[1:2, :] * hits[1]
    spread_columns = jnp.where(
        floor_div(iota((64, 768), 1), SLOTS) == iota((64, 768), 0), 1.0, 0.0
    ).astype(jnp.bfloat16)
    wanted = iota((256, 768), 1)
    wanted = wanted - SLOTS * floor_div(wanted, SLOTS)
    mine = dot(jnp.transpose(key).astype(jnp.bfloat16), spread_columns) == wanted
    high = weights.astype(jnp.bfloat16)
    low = (weights - high.astype(jnp.float32)).astype(jnp.bfloat16)
    for part, target in ((high, m.mix_high), (low, m.mix_low)):
        turned = jnp.transpose(dot(expert_of, part)).astype(jnp.bfloat16)
        target[...] = jnp.where(mine, dot(turned, spread_columns), 0.0).astype(jnp.bfloat16)

    for copy in own_copies[5:]:
        copy.wait()
    gate_near.forward()
    up_near.forward()
    down_near[0].forward()
    down_near[1].start()
    down_near[2].start()
    states_second(m)

    def gather(half):
        half_bytes(m.sent, m.landed, half, m.dispatch_sems.at[half], m.dispatch_sems.at[2 + half]).wait()
        unpack_half(m.landed, m.rows, matrix, half, 0, 512)

    def activate(half, first, last):
        def one(j, unused):
            rows = m.rows[half * 384 : (half + 1) * 384, :]
            opened = dot(rows, m.gate_slots[j])
            raised = dot(rows, m.up_slots[j])
            m.hidden[j, half * 384 : (half + 1) * 384, :] = (jax.nn.silu(opened) * raised).astype(
                jnp.bfloat16
            )
            return unused

        lax.fori_loop(first, last, one, 0)

    answers = (m.answers_0, m.answers_1, m.answers_2, m.answers_3)
    returned = (m.returned_0, m.returned_1, m.returned_2, m.returned_3)

    def answer(half, p):
        inside = slice(half * 384, (half + 1) * 384)
        start, size = CHUNKS[p]

        def one(n, unused):
            lines = pl.ds(pl.multiple_of(start + n * 256, 256), 256)
            total = jnp.zeros((384, 256), jnp.float32)
            for j in range(4):
                total = total + lax.dot_general(
                    m.hidden[j, inside],
                    m.down_slots[j, lines, :],
                    CONTRACT_LAST,
                    preferred_element_type=jnp.float32,
                )
            m.rows[inside, lines] = total.astype(jnp.bfloat16)
            return unused

        lax.fori_loop(0, size // 256, one, 0)
        for g in range(half * 8, half * 8 + 8):
            answers[p][g * 4 : g * 4 + 4] = pack_group(
                m.rows[g * 48 : (g + 1) * 48, start : start + size], matrix, size // 4
            )
        which = 2 * p + half
        sems = (m.answer_send.at[which], m.answer_recv.at[which])
        if half == 0:
            returned[p][7] = answers[p][7]
            send_group(answers[p], returned[p], 0, *sems, -1)

        def some(dxc, unused):
            send_group(answers[p], returned[p], dxc, *sems, -1)
            return unused

        lax.fori_loop(max(1, half * 4), half * 4 + 4, some, 0)

    gather(0)
    activate(0, 0, 3)
    gate_near.arrive()
    up_near.arrive()
    activate(0, 3, 4)
    down_near[0].arrive()
    answer(0, 0)
    gather(1)
    activate(1, 0, 4)
    answer(1, 0)
    states_third(m)
    down_near[1].forward()
    down_near[3].start()
    down_near[1].arrive()
    answer(0, 1)
    answer(1, 1)
    down_near[2].forward()
    down_near[3].forward()
    down_near[2].arrive()
    answer(0, 2)
    answer(1, 2)
    down_near[3].arrive()
    answer(0, 3)
    answer(1, 3)
    mixer_finish(m)

    for p, (start, size) in enumerate(CHUNKS):
        lines = pl.ds(start, size)
        for half in range(2):
            which = 2 * p + half
            half_bytes(
                answers[p], returned[p], half, m.answer_send.at[which], m.answer_recv.at[which]
            ).wait()
            unpack_half(returned[p], m.rows, matrix, half, start, size // 4)
            inside = slice(half * 384, (half + 1) * 384)
            share = dot(m.mix_high[:, inside], m.rows[inside, lines]) + dot(
                m.mix_low[:, inside], m.rows[inside, lines]
            )
            if half == 0:
                m.total[:, 0:size] = share
            else:
                m.routed_out[:, lines] = (m.total[:, 0:size] + share).astype(jnp.bfloat16)

    for near in [gate_near, up_near] + down_near:
        near.drain()
    for copy in tails:
        copy.wait_send()


def body(
    first_micro_values,
    group_state_maps,
    gate_preactivation,
    step_preactivation,
    head_step_bias,
    head_log_decay,
    decay_increment,
    head_direct_gain,
    convolution_value_taps,
    convolution_map_taps,
    grouped_norm_gain,
    second_micro_tokens,
    expert_norm_gain,
    routes,
    visit_weight,
    gate_weight_table,
    up_weight_table,
    down_weight_table,
):
    operands = (
        second_micro_tokens,
        expert_norm_gain.reshape(1, -1),
        routes.T,
        visit_weight.T,
        gate_weight_table,
        up_weight_table,
        down_weight_table,
        first_micro_values,
        group_state_maps,
        gate_preactivation,
        step_preactivation.T,
        decay_increment.T,
        head_step_bias.reshape(1, -1),
        head_log_decay.reshape(1, -1),
        head_direct_gain.reshape(1, -1),
        convolution_value_taps,
        convolution_map_taps,
        grouped_norm_gain.reshape(1, -1),
    )
    vmem = pl.BlockSpec(memory_space=pltpu.VMEM)
    hbm = pl.BlockSpec(memory_space=pl.ANY)
    return pl.pallas_call(
        kernel,
        out_shape=(
            jax.ShapeDtypeStruct((1024, 512), BF16),
            jax.ShapeDtypeStruct((256, 2048), BF16),
        ),
        in_specs=[hbm if name.endswith("_hbm") else vmem for name in INPUTS],
        out_specs=(vmem, vmem),
        scratch_shapes=list(SCRATCH.values()),
        compiler_params=pltpu.CompilerParams(
            collective_id=0, has_side_effects=True, vmem_limit_bytes=60 * 2**20
        ),
    )(*operands)


def solution(mesh):
    torus = Mesh(mesh.devices.reshape(8, 4, 2, mesh.shape["tp"]), ("ep_0", "ep_1", "ep_2", "tp"))
    in_specs = (
        P(EP, "tp"),
        P(None, EP, "tp"),
        P(EP, "tp"),
        P(EP, "tp"),
        P("tp"),
        P("tp"),
        P(EP, "tp"),
        P("tp"),
        P(None, "tp"),
        P(None, None, "tp"),
        P("tp"),
        P(EP_TP, None),
        P(),
        P(EP_TP, None),
        P(EP_TP, None),
        P(EP, None, "tp"),
        P(EP, None, "tp"),
        P(EP, None, "tp"),
    )
    out_specs = (P(EP, "tp"), P(EP_TP, None))
    return jax.shard_map(body, mesh=torus, in_specs=in_specs, out_specs=out_specs, check_vma=False)
```
